256 devices in a mesh: sp: 64 (over z, x, core), tp: 4 (over y).
Axes of the slice: x: 4, y: 4, z: 8, core: 2. Of those that a mesh axis runs over, the one named last changes fastest.
Arguments:
- residual: bfloat16 [24576, 2048], P('sp', 'tp'), may hold values from -6 to 6
- query_nope: bfloat16 [24576, 4096], P('sp', 'tp'), may hold values from -9 to 9
- query_rope: bfloat16 [24576, 2048], P('sp', 'tp'), may hold values from -600 to 600
- latent: bfloat16 [24576, 512], P('sp'), may hold values from -6 to 6
- rope_key: bfloat16 [24576, 64], P('sp'), may hold values from -6 to 6
- doc_ids: int32 [24576], P('sp'), may hold values from 0 to 31, never falling along the last dimension, each value on 1 to 1152 neighbouring positions
- key_up: bfloat16 [512, 4096], P(None, 'tp'), may hold values from -0.25 to 0.25
- value_up: bfloat16 [512, 4096], P(None, 'tp'), may hold values from -0.25 to 0.25
- out_proj: bfloat16 [4096, 2048], P('tp'), may hold values from -0.375 to 0.375
- norm1_gain: bfloat16 [2048], P('tp'), may hold values from 0.099609375 to 1.8984375
- norm1_bias: bfloat16 [2048], P('tp'), may hold values from -3 to 3
- ffn_gate: bfloat16 [2048, 5632], P('sp', 'tp'), may hold values from -0.125 to 0.125
- ffn_value: bfloat16 [2048, 5632], P('sp', 'tp'), may hold values from -0.125 to 0.125
- conv_gate: bfloat16 [3, 5632], P(None, 'tp'), may hold values from -3.5 to 3.5
- conv_value: bfloat16 [3, 5632], P(None, 'tp'), may hold values from -3.5 to 3.5
- ffn_down: bfloat16 [5632, 2048], P('tp', 'sp'), may hold values from -0.15625 to 0.15625
- norm2_gain: bfloat16 [2048], P('tp'), may hold values from 0.099609375 to 1.8984375
- norm2_bias: bfloat16 [2048], P('tp'), may hold values from -3 to 3
Outputs:
- layer_out: bfloat16 [24576, 2048], P('sp', 'tp')
The draws below stay inside these ranges and needn't reach their ends.
Inputs may be any that keep to these rules, and one draw needn't show every extreme that they name: `doc_ids`: document numbers never fall along the positions; each document holds 1 to 1152 positions, and one holds exactly 1152.
All inputs are finite; a program needn't handle non-finite values.
Results may differ from the reference program's by a relative error of at most 0.014.
Values may be sent and summed in bfloat16 or wider, within the bound.
A program may use at most 128 MiB of HBM per device.

```python
import math
import jax
import jax.numpy as jnp
import numpy as np
from jax import lax

D = 2048
HEADS = 32
NOPE = 128
ROPE = 64
VDIM = 128
LATENT = 512
FF = 5632
CONV = 3
REACH = 3
TOK_DEV = 384
TOKENS = 24576
DOCS = 32
N_SP = 64
N_TP = 4


def rope_base(key):
    base_rows = jnp.clip(jax.random.normal(jax.random.fold_in(key, 7), (TOKENS, ROPE), jnp.float32), -6.0, 6.0)
    return base_rows


def draw_rope_key(key, part):
    return rope_base(key).astype(jnp.bfloat16)


def draw_query_rope(key, part):
    drawn = jnp.clip(jax.random.normal(jax.random.fold_in(key, 9), (TOKENS, HEADS * ROPE), jnp.float32), -6.0, 6.0) * 1.5
    return drawn.astype(jnp.bfloat16)


def shard_levels(own_key, extent, cuts, low, largest):
    gain = 1.0
    for dim, shards_of in cuts:
        draws = jax.random.uniform(jax.random.fold_in(jax.random.fold_in(own_key, 6), dim), (shards_of,), jnp.float32, low / len(cuts), largest / len(cuts))
        gain = gain * jnp.repeat(jnp.exp(draws), extent[dim] // shards_of).reshape((-1,) + (1,) * (len(extent) - 1 - dim))
    return gain


def profile(number_of, total, most, lean):
    loads = [(1 << 20) // math.isqrt(rank ** lean) + 1 for rank in range(2, number_of + 1)]
    spare, counts = total - most - (number_of - 1), [1] * (number_of - 1)
    while spare > 0:
        candidates = [i for i in range(number_of - 1) if counts[i] < most]
        whole, remaining = sum([loads[i] for i in candidates]), spare
        for i in candidates:
            extra = min(most - counts[i], max(1, remaining * loads[i] // whole), spare)
            counts[i] = counts[i] + extra
            spare = spare - extra
    return np.array([most] + counts)


def ragged_sizes(own_key, count, total, most, skew):
    if count == 2:
        one = jax.random.randint(own_key, (), max(1, total - most), min(most, total - 1) + 1)
        return jnp.stack([one, total - one])
    lengths = jnp.asarray(profile(count, total, most, skew), jnp.int32)
    pairs = (count - 1) // 2
    donor, sink = lengths[1:1 + 2 * pairs:2], lengths[2:2 + 2 * pairs:2]
    room = jnp.minimum(donor - 1, most - sink)
    shifted = jax.random.randint(jax.random.fold_in(own_key, 1), (pairs,), 0, 1 << 20) % (room + 1)
    lengths = lengths.at[1:1 + 2 * pairs:2].set(donor - shifted).at[2:2 + 2 * pairs:2].set(sink + shifted)
    return lengths[jax.random.permutation(jax.random.fold_in(own_key, 2), count)]


def noise(own_key, dims, scale, bound, split=(), kind=jnp.bfloat16):
    gain = shard_levels(own_key, dims, split, -0.22, 0.18) if split else 1.0
    values = jax.random.normal(own_key, dims, jnp.float32) * scale * gain
    return jnp.minimum(jnp.maximum(values, -bound), bound).astype(kind)


def setup_inputs(seed: int = 0) -> dict:
    key_of = jax.random.split(jax.random.key(seed), 19)
    residual = noise(key_of[0], (TOKENS, D), 1.0, 6.0, ((0, 64), (1, 4)))
    query_nope = noise(key_of[1], (TOKENS, HEADS * NOPE), 1.5, 9.0, ((0, 64), (1, 4)))
    query_rope = draw_query_rope(jax.random.fold_in(key_of[18], 71), 0)
    latent = noise(key_of[3], (TOKENS, LATENT), 1.0, 6.0, ((0, 64),))
    rope_key = draw_rope_key(jax.random.fold_in(key_of[18], 71), 0)
    doc_ids = jnp.searchsorted(jnp.cumsum(ragged_sizes(key_of[5], DOCS, TOKENS, REACH * TOK_DEV, 1)), jnp.arange(TOKENS), side="right").astype(jnp.int32)
    key_up = noise(key_of[6], (LATENT, HEADS * NOPE), LATENT ** -0.5, 0.25, ((1, 4),))
    value_up = noise(key_of[7], (LATENT, HEADS * VDIM), LATENT ** -0.5, 0.25, ((1, 4),))
    out_proj = noise(key_of[8], (HEADS * VDIM, D), (HEADS * VDIM // 16) ** -0.5, 0.375, ((0, 4),))
    norm1_gain = jnp.clip(1.0 + 0.18 * jax.random.normal(key_of[9], (D,), jnp.float32), 0.099609375, 1.8984375).astype(jnp.bfloat16)
    norm1_bias = noise(key_of[10], (D,), 0.5, 3.0, ((0, 4),))
    ffn_gate = noise(key_of[11], (D, FF), D ** -0.5, 0.125, ((0, 64), (1, 4)))
    ffn_value = noise(key_of[12], (D, FF), D ** -0.5, 0.125, ((0, 64), (1, 4)))
    conv_gate = noise(key_of[13], (CONV, FF), CONV ** -0.5, 3.5, ((1, 4),))
    conv_value = noise(key_of[14], (CONV, FF), CONV ** -0.5, 3.5, ((1, 4),))
    ffn_down = noise(key_of[15], (FF, D), (FF // 4) ** -0.5, 0.15625, ((0, 4), (1, 64)))
    norm2_gain = jnp.clip(1.0 + 0.18 * jax.random.normal(key_of[16], (D,), jnp.float32), 0.099609375, 1.8984375).astype(jnp.bfloat16)
    norm2_bias = noise(key_of[17], (D,), 0.5, 3.0, ((0, 4),))
    return dict(residual=residual, query_nope=query_nope, query_rope=query_rope, latent=latent, rope_key=rope_key, doc_ids=doc_ids, key_up=key_up, value_up=value_up, out_proj=out_proj, norm1_gain=norm1_gain, norm1_bias=norm1_bias, ffn_gate=ffn_gate, ffn_value=ffn_value, conv_gate=conv_gate, conv_value=conv_value, ffn_down=ffn_down, norm2_gain=norm2_gain, norm2_bias=norm2_bias)


norm_eps = 1e-05
residual_scale = 8.0 ** 0.25
rope_base_freq = 10000.0
masked_score = -1e+30

def tables(positions):
    frequencies = 1.0 / rope_base_freq ** (jnp.arange(0, ROPE, 2, dtype=jnp.float32) / ROPE)
    angles = positions.astype(jnp.float32)[:, None] * frequencies[None, :]
    return (jnp.cos(angles), jnp.sin(angles))

def rotate(vectors, cosine, sine_table):
    half_width = vectors.shape[-1] // 2
    front_half = vectors[..., :half_width]
    back_half = vectors[..., half_width:]
    return jnp.concatenate([front_half * cosine - back_half * sine_table, front_half * sine_table + back_half * cosine], axis=-1)

def layer_norm(mixed, gain_row, bias_row):
    width = mixed.shape[-1]
    row_mean = lax.optimization_barrier(jnp.sum(mixed, -1, keepdims=True)) / width
    row_power = lax.optimization_barrier(jnp.sum(mixed * mixed, -1, keepdims=True)) / width
    return (mixed - row_mean) * lax.rsqrt(row_power - row_mean * row_mean + norm_eps) * gain_row.astype(jnp.float32) + bias_row.astype(jnp.float32)

def reference(residual, query_nope, query_rope, latent, rope_key, doc_ids, key_up, value_up, out_proj, norm1_gain, norm1_bias, ffn_gate, ffn_value, conv_gate, conv_value, ffn_down, norm2_gain, norm2_bias):
    row_count = TOK_DEV
    window = (REACH + 1) * row_count
    lead_rows = REACH * row_count
    rim_rows = CONV - 1
    positions = jnp.arange(TOKENS, dtype=jnp.int32)
    cosine, sine_table = tables(positions)
    turned_key = rotate(rope_key.astype(jnp.float32), cosine, sine_table).astype(jnp.bfloat16)
    turned_query = rotate(query_rope.astype(jnp.float32).reshape(TOKENS, HEADS, ROPE), cosine[:, None], sine_table[:, None]).astype(jnp.bfloat16)
    padded_latent = jnp.concatenate([jnp.zeros((lead_rows, LATENT), jnp.bfloat16), latent], 0)
    padded_key = jnp.concatenate([jnp.zeros((lead_rows, ROPE), jnp.bfloat16), turned_key], 0)
    padded_doc = jnp.concatenate([jnp.full((lead_rows,), -1, jnp.int32), doc_ids], 0)
    head_group = HEADS * VDIM // N_TP
    scale = (NOPE + ROPE) ** (-0.5)

    def first_half(block_index):
        row_start = (block_index * row_count).astype(jnp.int32)
        own_pos = row_start + jnp.arange(row_count, dtype=jnp.int32)
        win_latent = lax.dynamic_slice_in_dim(padded_latent, row_start, window, 0)
        win_key = lax.dynamic_slice_in_dim(padded_key, row_start, window, 0)
        win_doc = lax.dynamic_slice_in_dim(padded_doc, row_start, window, 0)
        own_doc = lax.dynamic_slice_in_dim(doc_ids, row_start, row_count, 0)
        key_pos = row_start - lead_rows + jnp.arange(window, dtype=jnp.int32)
        allowed = (key_pos[None, :] <= own_pos[:, None]) & (key_pos[None, :] >= 0) & (win_doc[None, :] == own_doc[:, None])
        key_rows = jnp.dot(win_latent, key_up, preferred_element_type=jnp.float32).astype(jnp.bfloat16).reshape(window, HEADS, NOPE)
        values = jnp.dot(win_latent, value_up, preferred_element_type=jnp.float32).astype(jnp.bfloat16).reshape(window, HEADS, VDIM)
        queries = lax.dynamic_slice_in_dim(query_nope, row_start, row_count, 0).reshape(row_count, HEADS, NOPE)
        turned = lax.dynamic_slice_in_dim(turned_query, row_start, row_count, 0)
        scores = jnp.einsum('qhd,khd->hqk', queries.astype(jnp.float32), key_rows.astype(jnp.float32))
        scores = scores + jnp.einsum('qhr,kr->hqk', turned.astype(jnp.float32), win_key.astype(jnp.float32))
        scores = jnp.where(allowed[None], scores * scale, masked_score)
        row_max = lax.optimization_barrier(jnp.max(scores, -1, keepdims=True))
        weights = jnp.exp(scores - row_max)
        weights = (weights / lax.optimization_barrier(jnp.sum(weights, -1, keepdims=True))).astype(jnp.bfloat16)
        attended = jnp.einsum('hqk,khd->qhd', weights.astype(jnp.float32), values.astype(jnp.float32)).astype(jnp.bfloat16).reshape(row_count, HEADS * VDIM)
        projected = jnp.zeros((row_count, D), jnp.float32)
        for member in range(N_TP):
            partial_value = jnp.dot(attended[:, member * head_group:(member + 1) * head_group], out_proj[member * head_group:(member + 1) * head_group], preferred_element_type=jnp.float32).astype(jnp.bfloat16)
            projected = projected + lax.optimization_barrier(partial_value).astype(jnp.float32)
        mixed = residual_scale * lax.dynamic_slice_in_dim(residual, row_start, row_count, 0).astype(jnp.float32) + projected
        return layer_norm(mixed, norm1_gain, norm1_bias).astype(jnp.bfloat16)
    normed = lax.map(first_half, jnp.arange(N_SP, dtype=jnp.int32)).reshape(TOKENS, D)
    padded_normed = jnp.concatenate([jnp.zeros((rim_rows, D), jnp.bfloat16), normed], 0)
    padded_doc_two = jnp.concatenate([jnp.full((rim_rows,), -1, jnp.int32), doc_ids], 0)
    unit_group = FF // N_TP

    def second_half(block_index):
        row_start = (block_index * row_count).astype(jnp.int32)
        own_pos = row_start + jnp.arange(row_count, dtype=jnp.int32)
        block_rows = lax.dynamic_slice_in_dim(padded_normed, row_start, row_count + rim_rows, 0)
        block_doc = lax.dynamic_slice_in_dim(padded_doc_two, row_start, row_count + rim_rows, 0)
        own_doc = block_doc[rim_rows:]
        gate_pre = jnp.dot(block_rows, ffn_gate, preferred_element_type=jnp.float32).astype(jnp.bfloat16)
        value_pre = jnp.dot(block_rows, ffn_value, preferred_element_type=jnp.float32).astype(jnp.bfloat16)
        gate_mix = jnp.zeros((row_count, FF), jnp.float32)
        value_mix = jnp.zeros((row_count, FF), jnp.float32)
        for tap_index in range(CONV):
            valid_tap = ((block_doc[tap_index:tap_index + row_count] == own_doc) & (own_pos - rim_rows + tap_index >= 0)).astype(jnp.float32)[:, None]
            gate_mix = gate_mix + conv_gate[tap_index].astype(jnp.float32) * gate_pre[tap_index:tap_index + row_count].astype(jnp.float32) * valid_tap
            value_mix = value_mix + conv_value[tap_index].astype(jnp.float32) * value_pre[tap_index:tap_index + row_count].astype(jnp.float32) * valid_tap
        hidden = (value_mix * jax.nn.gelu(gate_mix)).astype(jnp.bfloat16)
        ffn_out = jnp.zeros((row_count, D), jnp.float32)
        for member in range(N_TP):
            partial_value = jnp.dot(hidden[:, member * unit_group:(member + 1) * unit_group], ffn_down[member * unit_group:(member + 1) * unit_group], preferred_element_type=jnp.float32).astype(jnp.bfloat16)
            ffn_out = ffn_out + lax.optimization_barrier(partial_value).astype(jnp.float32)
        mixed = residual_scale * block_rows[rim_rows:].astype(jnp.float32) + ffn_out
        return layer_norm(mixed, norm2_gain, norm2_bias).astype(jnp.bfloat16)
    return lax.map(second_half, jnp.arange(N_SP, dtype=jnp.int32)).reshape(TOKENS, D)
```

```python
import jax
import jax.numpy as jnp
from jax import lax
from jax.experimental import pallas as pl
from jax.experimental.pallas import tpu as pltpu
from jax.sharding import PartitionSpec as P

D = 2048
NOPE = 128
ROPE = 64
VDIM = 128
CONV = 3
REACH = 3

norm_eps = 1e-05
residual_scale = 8.0**0.25
rope_base_freq = 10000.0
masked_score = -1e30
SCALE2 = (NOPE + ROPE) ** (-0.5) * 1.4426950408889634

NX, NZ, NY = 4, 8, 4
ROWS = 384
HALF = ROWS // 2
CH = 512
UNITS = 1408
DA = 512
LA = DA + UNITS
LW = 3 * UNITS
PACKW = 640
PACKR = 400
MESH = pl.DeviceIdType.MESH
BF = jnp.bfloat16
F32 = jnp.float32


def dot(a, b):
    return jnp.dot(a, b, preferred_element_type=F32)


def dot_nt(a, b):
    return lax.dot_general(a, b, (((1,), (1,)), ((), ())), preferred_element_type=F32)


def layer_kernel(
    pack_h, qn_h, qr_h, kup_h, vup_h, op_h, res_h, wsh_h, gb_ref, cv_ref,
    out_ref,
    packs, qn, qr, kup, vup, op, res, w, gbs, att, acc, mrun, lrun, dcol,
    sa, sp_buf, sm_buf, pfp, pfm, own, ra, rb, ra2, rb2, m4, nf, gv, hid, stat, stats,
    lsem, ssem, rsem,
):
    sp = lax.axis_index("sp")
    y = lax.axis_index("tp")
    c = lax.rem(sp, 2)
    k = lax.div(sp, 2)
    x = lax.rem(k, NX)
    z = lax.div(k, NX)

    def wrap(v, n):
        return lax.rem(v + n, n)

    def dev(zz, xx, cc, yy):
        return ((wrap(zz, NZ) * NX + wrap(xx, NX)) * 2 + cc, wrap(yy, NY))

    def chip(kk, cc):
        return (wrap(kk, NZ * NX) * 2 + cc, y)

    xp, xm = dev(z, x + 1, c, y), dev(z, x - 1, c, y)
    zp, zm = dev(z + 1, x, c, y), dev(z - 1, x, c, y)
    sib = dev(z, x, 1 - c, y)
    yp, ym, yy = dev(z, x, c, y + 1), dev(z, x, c, y - 1), dev(z, x, c, y + 2)
    nextc, prevc = chip(k + 1, c), chip(k - 1, c)
    nexto, prevo = chip(k + 1, 1 - c), chip(k - 1, 1 - c)

    local = []
    def fetch(src, dst):
        d = pltpu.make_async_copy(src, dst, lsem.at[len(local)])
        d.start()
        local.append(d)
        return d
    f_pack = fetch(pack_h, packs.at[0])
    f_w = fetch(wsh_h, w.at[z, x, c])
    f_kup = fetch(kup_h, kup)
    f_qn = fetch(qn_h, qn)
    f_qr = fetch(qr_h, qr)
    f_vup = fetch(vup_h, vup)
    f_op = fetch(op_h, op)
    f_res = fetch(res_h, res)

    barrier = pltpu.get_barrier_semaphore()
    peers = (xp, xm, zp, zm, sib, yp, ym, yy, nextc, prevc, nexto, prevo)
    for p in peers:
        pl.semaphore_signal(barrier, inc=1, device_id=p, device_id_type=MESH)
    pl.semaphore_wait(barrier, len(peers))

    sends = []
    names = {}

    def rid(name):
        return names.setdefault(name, len(names))

    def copy_to(src, dst, to, name):
        d = pltpu.make_async_remote_copy(
            src_ref=src, dst_ref=dst, send_sem=ssem.at[len(sends)],
            recv_sem=rsem.at[rid(name)], device_id=to, device_id_type=MESH,
        )
        sends.append(d)
        return d

    def send(src, dst, to, name):
        copy_to(src, dst, to, name).start()

    def arrive(dst, name):
        pltpu.make_async_remote_copy(
            src_ref=dst, dst_ref=dst, send_sem=ssem.at[0],
            recv_sem=rsem.at[rid(name)], device_id=sib, device_id_type=MESH,
        ).wait_recv()

    def wa(dz, dx):
        return w.at[wrap(z + dz, NZ), wrap(x + dx, NX), c, :, pl.ds(0, LA)]

    def za(dz, cc, lo=0, n=NX):
        return w.at[wrap(z + dz, NZ), pl.ds(lo, n), cc, :, pl.ds(0, LA)]

    def wb(dz, lo=LA, n=LW - LA):
        return w.at[wrap(z + dz, NZ), x, c, :, pl.ds(lo, n)]

    def xb(dx, cc, lo=0, n=NZ):
        return w.at[pl.ds(lo, n), wrap(x + dx, NX), cc, :, pl.ds(LA, LW - LA)]

    BH = (LW - LA) // 2
    HZ = NZ // 2
    HX = NX // 2

    def same(ref, to, name):
        send(ref, ref, to, name)

    def a_start():
        same(wa(0, 0), xp, "a1m")
        same(wa(0, 0), xm, "a1p")

    def a_one():
        arrive(wa(0, 1), "a1p")
        same(wa(0, 1), xm, "a2p")

    def a_two():
        arrive(wa(0, -1), "a1m")
        arrive(wa(0, 2), "a2p")
        same(za(0, c), zp, "z1m")
        same(za(0, c), zm, "z1p")
        same(za(0, c), sib, "sz0")

    def a_step(s):
        arrive(za(-s, c), f"z{s}m")
        arrive(za(s, c), f"z{s}p")
        if s < 3:
            same(za(-s, c), zp, f"z{s + 1}m")
            same(za(s, c), zm, f"z{s + 1}p")
        else:
            same(za(-s, c, 0, HX), zp, "z4m")
            same(za(s, c, HX, HX), zm, "z4p")
        same(za(-s, c), sib, f"sz{s}m")
        same(za(s, c), sib, f"sz{s}p")

    def a_last():
        arrive(za(4, c, 0, HX), "z4m")
        arrive(za(4, c, HX, HX), "z4p")
        same(za(4, c), sib, "sz4")

    def a_done():
        arrive(za(0, 1 - c), "sz0")
        for s in (1, 2, 3):
            arrive(za(-s, 1 - c), f"sz{s}m")
            arrive(za(s, 1 - c), f"sz{s}p")
        arrive(za(4, 1 - c), "sz4")

    def b_start():
        same(wb(0), zp, "b1m")
        same(wb(0), zm, "b1p")

    def b_step(s):
        arrive(wb(-s), f"b{s}m")
        arrive(wb(s), f"b{s}p")
        if s < 3:
            same(wb(-s), zp, f"b{s + 1}m")
            same(wb(s), zm, f"b{s + 1}p")
        else:
            same(wb(-s, LA, BH), zp, "b4m")
            same(wb(s, LA + BH, BH), zm, "b4p")

    def b_turn():
        arrive(wb(4, LA, BH), "b4m")
        arrive(wb(4, LA + BH, BH), "b4p")
        same(xb(0, c), xp, "x1m")
        same(xb(0, c), xm, "x1p")
        same(xb(0, c), sib, "sx0")

    def b_cross():
        arrive(xb(-1, c), "x1m")
        arrive(xb(1, c), "x1p")
        same(xb(-1, c, 0, HZ), xp, "x2m")
        same(xb(1, c, HZ, HZ), xm, "x2p")
        same(xb(-1, c), sib, "sx1m")
        same(xb(1, c), sib, "sx1p")

    def b_last():
        arrive(xb(2, c, 0, HZ), "x2m")
        arrive(xb(2, c, HZ, HZ), "x2p")
        same(xb(2, c), sib, "sx2")

    def b_done():
        arrive(xb(0, 1 - c), "sx0")
        arrive(xb(-1, 1 - c), "sx1m")
        arrive(xb(1, 1 - c), "sx1p")
        arrive(xb(2, 1 - c), "sx2")

    f_w.wait()
    a_start()
    b_start()
    f_pack.wait()
    third_at = len(sends)
    third = copy_to(packs.at[0], packs.at[1], sib, "l1")

    @pl.when(c == 0)
    def _():
        third.start()

    send(packs.at[0], packs.at[2], nextc, "l2")
    send(gb_ref, gbs.at[y], yp, "gm")
    send(gb_ref, gbs.at[y], ym, "gp")
    send(gb_ref, gbs.at[y], yy, "g2")

    def doc_column(slot):
        return packs[slot, 0:ROWS, 512:640].astype(F32)[:, ROPE : ROPE + 1]

    dcol[8 : 8 + ROWS, :] = jnp.broadcast_to(doc_column(0), (ROWS, 128))

    def attend(slot, back, kind, first=False, last=False):
        exists = sp >= back

        def body(pair, carry):
            off = pl.multiple_of(pair * 256, 256)
            lat = packs[slot, 0:ROWS, 0:512]
            kr = packs[slot, 0:ROWS, 512:640]
            kdoc = packs[slot, ROWS:PACKR, 0:ROWS].astype(F32)[0:1, :]
            kdoc = jnp.where(exists, kdoc, -1.0)
            k2 = dot(lat, kup[:, pl.ds(off, 256)]).astype(BF)
            v2 = dot(lat, vup[:, pl.ds(off, 256)]).astype(BF)
            for hh in range(2):
                h = pair * 2 + hh
                lanes = pl.ds(pl.multiple_of(off + hh * 128, 128), 128)
                kk = jnp.concatenate([k2[:, hh * 128 : hh * 128 + 128], kr], axis=1)
                vv = v2[:, hh * 128 : hh * 128 + 128]
                for qi in range(3):
                    r0 = qi * 128
                    rows = pl.ds(r0, 128)
                    lo, hi = 0, ROWS
                    if kind == "diag":
                        hi = r0 + 128
                    if kind == "far":
                        lo = r0
                    q = jnp.concatenate([qn[rows, lanes], qr[rows, lanes]], axis=1)
                    s = dot_nt(q, kk[lo:hi])
                    qdoc = dcol[8 + r0 : 8 + r0 + 128, 0:1]
                    ok = qdoc == kdoc[:, lo:hi]
                    if kind == "diag":
                        qi_pos = lax.broadcasted_iota(jnp.int32, s.shape, 0) + r0
                        ki_pos = lax.broadcasted_iota(jnp.int32, s.shape, 1)
                        ok = ok & (ki_pos <= qi_pos)
                    s = jnp.where(ok, s, masked_score)
                    mx = jnp.max(s, axis=1, keepdims=True)
                    if first:
                        p = jnp.exp2((s - mx) * SCALE2)
                        total = jnp.broadcast_to(jnp.sum(p, axis=1, keepdims=True), (128, 128))
                        o = dot(p.astype(BF), vv[lo:hi])
                        mnew = jnp.broadcast_to(mx, (128, 128))
                    else:
                        mold = mrun[h, rows, :]
                        mnew = jnp.maximum(mold, mx)
                        alpha = jnp.exp2((mold - mnew) * SCALE2)
                        p = jnp.exp2((s - mnew[:, 0:1]) * SCALE2)
                        total = lrun[h, rows, :] * alpha + jnp.sum(p, axis=1, keepdims=True)
                        o = acc[h, rows, :] * alpha + dot(p.astype(BF), vv[lo:hi])
                    if last:
                        att[rows, lanes] = (o / total).astype(BF)
                    else:
                        mrun[h, rows, :] = mnew
                        lrun[h, rows, :] = total
                        acc[h, rows, :] = o
            return carry

        lax.fori_loop(0, 4, body, 0)

    f_kup.wait()
    f_qn.wait()
    f_qr.wait()
    f_vup.wait()
    attend(0, 0, "diag", first=True)
    a_one()
    b_step(1)
    a_two()
    b_step(2)
    b_step(3)
    arrive(packs.at[2], "l2")
    hand = copy_to(packs.at[2], packs.at[3 - 2 * c], sib, "l1")
    hand_three = pltpu.make_async_remote_copy(
        src_ref=packs.at[2], dst_ref=packs.at[3], send_sem=ssem.at[len(sends) - 1],
        recv_sem=rsem.at[rid("l3")], device_id=sib, device_id_type=MESH,
    )
    relay = pltpu.make_async_remote_copy(
        src_ref=packs.at[2], dst_ref=packs.at[3], send_sem=ssem.at[third_at],
        recv_sem=rsem.at[rid("l3")], device_id=nexto, device_id_type=MESH,
    )
    hand_one = pltpu.make_async_remote_copy(
        src_ref=packs.at[2], dst_ref=packs.at[1], send_sem=ssem.at[len(sends) - 1],
        recv_sem=rsem.at[rid("l1")], device_id=sib, device_id_type=MESH,
    )

    @pl.when(c == 0)
    def _():
        hand_three.start()

    @pl.when(c == 1)
    def _():
        hand_one.start()
        relay.start()

    attend(2, 2, "full")
    b_turn()
    arrive(packs.at[1], "l1")
    before = jnp.where(sp >= 1, doc_column(1)[ROWS - 8 : ROWS, :], -1.0)
    dcol[0:8, :] = jnp.broadcast_to(before, (8, 128))
    attend(1, 1, "full")
    arrive(packs.at[3], "l3")
    attend(3, 3, "far", last=True)
    a_step(1)

    def shared_sum(chunk, tag, ra, rb, pump_one, pump_two):
        f = chunk(wrap(y + 2, NY))
        sa[...] = f.astype(BF)
        send(sa.at[pl.ds(0, HALF)], ra.at[0], yp, tag + "am")
        send(sa.at[pl.ds(HALF, HALF)], ra.at[1], ym, tag + "ap")
        f = chunk(wrap(y + 1, NY))
        pfp[...] = f[:HALF]
        sp_buf[pl.ds(HALF, HALF), :] = f[HALF:].astype(BF)
        send(sp_buf.at[pl.ds(HALF, HALF)], rb.at[0, pl.ds(HALF, HALF)], yp, tag + "bm1")
        f = chunk(wrap(y - 1, NY))
        pfm[...] = f[HALF:]
        sm_buf[pl.ds(0, HALF), :] = f[:HALF].astype(BF)
        send(sm_buf.at[pl.ds(0, HALF)], rb.at[1, pl.ds(0, HALF)], ym, tag + "bp0")
        own[...] = chunk(y)
        pump_one()
        arrive(ra.at[0], tag + "am")
        sp_buf[pl.ds(0, HALF), :] = (pfp[...] + ra[0].astype(F32)).astype(BF)
        send(sp_buf.at[pl.ds(0, HALF)], rb.at[0, pl.ds(0, HALF)], yp, tag + "bm0")
        arrive(ra.at[1], tag + "ap")
        sm_buf[pl.ds(HALF, HALF), :] = (pfm[...] + ra[1].astype(F32)).astype(BF)
        send(sm_buf.at[pl.ds(HALF, HALF)], rb.at[1, pl.ds(HALF, HALF)], ym, tag + "bp1")
        pump_two()
        arrive(rb.at[0, pl.ds(HALF, HALF)], tag + "bm1")
        arrive(rb.at[1, pl.ds(0, HALF)], tag + "bp0")
        arrive(rb.at[0, pl.ds(0, HALF)], tag + "bm0")
        arrive(rb.at[1, pl.ds(HALF, HALF)], tag + "bp1")
        return own[...] + rb[0].astype(F32) + rb[1].astype(F32)

    def settle(ds):
        for d in ds:
            d.wait_send()

    f_op.wait()
    f_res.wait()

    def head_share(t):
        return dot(att[...], op[:, pl.ds(pl.multiple_of(t * CH, CH), CH)])

    mark = len(sends)
    total_one = shared_sum(head_share, "p", ra, rb, lambda: None, lambda: a_step(2))
    m4[y] = (residual_scale * res[...].astype(F32) + total_one).astype(BF)

    def piece(dy, lo):
        return m4.at[wrap(y + dy, NY), pl.ds(lo, HALF)]

    same(piece(0, 0), yp, "m1m0")
    same(piece(0, HALF), ym, "m1p1")
    same(piece(0, HALF), yp, "m1m1")
    same(piece(0, 0), ym, "m1p0")
    b_cross()
    arrive(piece(-1, 0), "m1m0")
    same(piece(-1, 0), yp, "m2m")
    arrive(piece(1, HALF), "m1p1")
    same(piece(1, HALF), ym, "m2p")
    arrive(gbs.at[wrap(y - 1, NY)], "gm")
    arrive(gbs.at[wrap(y + 1, NY)], "gp")
    arrive(gbs.at[wrap(y + 2, NY)], "g2")
    gbs[y] = gb_ref[...]
    a_step(3)
    arrive(piece(-1, HALF), "m1m1")
    arrive(piece(1, 0), "m1p0")
    arrive(piece(2, 0), "m2m")
    arrive(piece(2, HALF), "m2p")

    def norm_rows(i, carry):
        rows = pl.ds(pl.multiple_of(i * 32, 32), 32)
        parts = [m4[t, rows, :].astype(F32) for t in range(NY)]
        s = sum(jnp.sum(v, axis=1, keepdims=True) for v in parts) / D
        q = sum(jnp.sum(v * v, axis=1, keepdims=True) for v in parts) / D
        r = lax.rsqrt(q - s * s + norm_eps)
        for t in range(NY):
            nf[rows, t * CH : (t + 1) * CH] = (
                (parts[t] - s) * r * gbs[t, 0:1, :] + gbs[t, 1:2, :]
            ).astype(BF)
        return carry

    lax.fori_loop(0, ROWS // 32, norm_rows, 0)
    b_last()
    a_last()
    b_done()
    a_done()

    def up(j, carry):
        lanes = pl.ds(pl.multiple_of(DA + j * 256, 128), 256)
        f = dot(nf[...], w[:, :, :, :, lanes].reshape(D, 256))
        gv[8 : 8 + ROWS, pl.ds(pl.multiple_of(j * 256, 256), 256)] = f
        return carry

    lax.fori_loop(0, 2 * UNITS // 256, up, 0)
    tail = pl.ds(ROWS, 8)

    to_sib = copy_to(gv.at[tail], stat.at[0], sib, "t")
    to_next = pltpu.make_async_remote_copy(
        src_ref=gv.at[tail], dst_ref=stat.at[0], send_sem=ssem.at[len(sends) - 1],
        recv_sem=rsem.at[rid("t")], device_id=nexto, device_id_type=MESH,
    )

    @pl.when(c == 0)
    def _():
        to_sib.start()

    @pl.when(c == 1)
    def _():
        to_next.start()

    def conv_block(r0):
        here = dcol[8 + r0 : 8 + r0 + 128, :]
        one = (dcol[7 + r0 : 7 + r0 + 128, :] == here).astype(F32)
        two = (dcol[6 + r0 : 6 + r0 + 128, :] == here).astype(F32)

        def cols(j, carry):
            def mix(base):
                lanes = pl.ds(pl.multiple_of(base + j * 128, 128), 128)
                a0 = gv[6 + r0 : 6 + r0 + 128, lanes]
                a1 = gv[7 + r0 : 7 + r0 + 128, lanes]
                a2 = gv[8 + r0 : 8 + r0 + 128, lanes]
                return (
                    cv_ref[0:1, lanes] * a0 * two
                    + cv_ref[1:2, lanes] * a1 * one
                    + cv_ref[2:3, lanes] * a2
                )

            g = mix(0)
            v = mix(UNITS)
            act = 0.5 * g * (1.0 + jnp.tanh(0.7978845608028654 * (g + 0.044715 * (g * g * g))))
            hid[r0 : r0 + 128, pl.ds(pl.multiple_of(j * 128, 128), 128)] = (v * act).astype(BF)
            return carry

        lax.fori_loop(0, UNITS // 128, cols, 0)

    conv_block(256)
    conv_block(128)
    arrive(stat.at[0], "t")
    gv[0:8, :] = jnp.where(sp >= 1, stat[0], 0.0)
    conv_block(0)

    def unit_share(t):
        rows = pl.ds(2 * t, 2)
        da = w[rows, :, :, :, 0:DA].reshape(CH, DA)
        db = w[rows, :, :, :, LA + UNITS : LW].reshape(CH, UNITS - DA)
        return dot_nt(hid[:, 0:DA], da) + dot_nt(hid[:, DA:UNITS], db)

    settle(sends[mark : mark + 6])
    total_two = shared_sum(unit_share, "u", ra2, rb2, lambda: None, lambda: None)
    mixed = (
        residual_scale * nf[:, pl.ds(pl.multiple_of(y * CH, CH), CH)].astype(F32) + total_two
    )
    own[...] = mixed
    lane = lax.broadcasted_iota(jnp.int32, (ROWS, 128), 1)
    s = jnp.sum(mixed, axis=1, keepdims=True)
    q = jnp.sum(mixed * mixed, axis=1, keepdims=True)
    both = jnp.where(lane == 0, s, jnp.where(lane == 1, q, 0.0))
    stats[y] = both.T[0:8, :]
    same(stats.at[y], yp, "qm")
    same(stats.at[y], ym, "qp")
    same(stats.at[y], yy, "q2")
    arrive(stats.at[wrap(y - 1, NY)], "qm")
    arrive(stats.at[wrap(y + 1, NY)], "qp")
    arrive(stats.at[wrap(y + 2, NY)], "q2")
    tot = (stats[0] + stats[1]) + (stats[2] + stats[3])
    back = jnp.concatenate([tot, jnp.zeros((120, ROWS), F32)], axis=0).T
    s = back[:, 0:1] / D
    q = back[:, 1:2] / D
    r = lax.rsqrt(q - s * s + norm_eps)
    out_ref[...] = ((own[...] - s) * r * gb_ref[2:3, :] + gb_ref[3:4, :]).astype(BF)
    settle(sends[:mark])
    settle(sends[mark + 6 :])


N_SEND = 72
N_RECV = 72


def tables(positions):
    frequencies = 1.0 / rope_base_freq ** (jnp.arange(0, ROPE, 2, dtype=jnp.float32) / ROPE)
    angles = positions.astype(jnp.float32)[:, None] * frequencies[None, :]
    return (jnp.cos(angles), jnp.sin(angles))


def rotate(vectors, cosine, sine_table):
    half_width = vectors.shape[-1] // 2
    front_half = vectors[..., :half_width]
    back_half = vectors[..., half_width:]
    return jnp.concatenate(
        [
            front_half * cosine - back_half * sine_table,
            front_half * sine_table + back_half * cosine,
        ],
        axis=-1,
    )


def local(
    residual, query_nope, query_rope, latent, rope_key, doc_ids, key_up, value_up, out_proj,
    norm1_gain, norm1_bias, ffn_gate, ffn_value, conv_gate, conv_value, ffn_down,
    norm2_gain, norm2_bias,
):
    rows = latent.shape[0]
    heads = query_nope.shape[1] // NOPE
    positions = lax.axis_index("sp") * rows + jnp.arange(rows, dtype=jnp.int32)
    cosine, sine = tables(positions)
    turned_key = rotate(rope_key.astype(F32), cosine, sine).astype(BF)
    turned_query = rotate(
        query_rope.astype(F32).reshape(rows, heads, ROPE), cosine[:, None], sine[:, None]
    ).astype(BF)
    turned_query = jnp.pad(turned_query, ((0, 0), (0, 0), (0, 128 - ROPE))).reshape(rows, heads * 128)
    doc = doc_ids.astype(BF)
    body = jnp.concatenate(
        [latent, turned_key, doc[:, None], jnp.zeros((rows, PACKW - 577), BF)], axis=1
    )
    foot = jnp.pad(doc[None, :], ((0, PACKR - rows - 1), (0, PACKW - rows)))
    pack = jnp.concatenate([body, foot], axis=0)
    down = ffn_down.T
    shard = jnp.concatenate([down[:, :DA], ffn_gate, ffn_value, down[:, DA:]], axis=1)
    gains = jnp.stack([norm1_gain, norm1_bias, norm2_gain, norm2_bias]).astype(F32)
    gains = jnp.pad(gains, ((0, 4), (0, 0)))
    taps = jnp.pad(jnp.concatenate([conv_gate, conv_value], axis=1).astype(F32), ((0, 5), (0, 0)))

    anyspec = pl.BlockSpec(memory_space=pl.ANY)
    vspec = pl.BlockSpec(memory_space=pltpu.VMEM)
    V = pltpu.VMEM
    return pl.pallas_call(
        layer_kernel,
        out_shape=jax.ShapeDtypeStruct((rows, CH), BF),
        in_specs=[anyspec] * 8 + [vspec] * 2,
        out_specs=vspec,
        scratch_shapes=[
            V((4, PACKR, PACKW), BF),
            V((ROWS, 1024), BF),
            V((ROWS, 1024), BF),
            V((512, 1024), BF),
            V((512, 1024), BF),
            V((1024, D), BF),
            V((ROWS, CH), BF),
            V((NZ, NX, 2, 32, LW), BF),
            V((NY, 8, CH), F32),
            V((ROWS, 1024), BF),
            V((8, ROWS, 128), F32),
            V((8, ROWS, 128), F32),
            V((8, ROWS, 128), F32),
            V((8 + ROWS, 128), F32),
            V((ROWS, CH), BF),
            V((ROWS, CH), BF),
            V((ROWS, CH), BF),
            V((HALF, CH), F32),
            V((HALF, CH), F32),
            V((ROWS, CH), F32),
            V((2, HALF, CH), BF),
            V((2, ROWS, CH), BF),
            V((2, HALF, CH), BF),
            V((2, ROWS, CH), BF),
            V((NY, ROWS, CH), BF),
            V((ROWS, D), BF),
            V((8 + ROWS, 2 * UNITS), F32),
            V((ROWS, UNITS), BF),
            V((1, 8, 2 * UNITS), F32),
            V((NY, 8, ROWS), F32),
            pltpu.SemaphoreType.DMA((8,)),
            pltpu.SemaphoreType.DMA((N_SEND,)),
            pltpu.SemaphoreType.DMA((N_RECV,)),
        ],
        compiler_params=pltpu.CompilerParams(
            collective_id=0, has_side_effects=True, vmem_limit_bytes=60 * 1024 * 1024
        ),
    )(pack, query_nope, turned_query, key_up, value_up, out_proj, residual, shard, gains, taps)


def solution(mesh):
    placed = (
        P("sp", "tp"),
        P("sp", "tp"),
        P("sp", "tp"),
        P("sp", None),
        P("sp", None),
        P("sp"),
        P(None, "tp"),
        P(None, "tp"),
        P("tp", None),
        P("tp"),
        P("tp"),
        P("sp", "tp"),
        P("sp", "tp"),
        P(None, "tp"),
        P(None, "tp"),
        P("tp", "sp"),
        P("tp"),
        P("tp"),
    )
    return jax.shard_map(
        local, mesh=mesh, in_specs=placed, out_specs=P("sp", "tp"), check_vma=False
    )
```

```python
import jax
import jax.numpy as jnp
from jax import lax
from jax.experimental import pallas as pl
from jax.experimental.pallas import tpu as pltpu
from jax.sharding import PartitionSpec as P

D = 2048
NOPE = 128
ROPE = 64
VDIM = 128
CONV = 3
REACH = 3

norm_eps = 1e-05
residual_scale = 8.0**0.25
rope_base_freq = 10000.0
masked_score = -1e30
SCALE2 = (NOPE + ROPE) ** (-0.5) * 1.4426950408889634

NX, NZ, NY = 4, 8, 4
ROWS = 384
HALF = ROWS // 2
CH = 512
UNITS = 1408
DA = 512
LA = DA + UNITS
LW = 3 * UNITS
PACKW = 640
GROUP = 4
N_SEND = 96
N_RECV = 96
S_ALT = N_SEND - 4
MESH = pl.DeviceIdType.MESH
BF = jnp.bfloat16
F32 = jnp.float32


def dot(a, b):
    return jnp.dot(a, b, preferred_element_type=F32)


def dot_nt(a, b):
    return lax.dot_general(a, b, (((1,), (1,)), ((), ())), preferred_element_type=F32)


def layer_kernel(
    lat_h, qn_h, qr_h, kup_h, vup_h, op_h, res_h, gate_h, value_h, down_h,
    key_ref, cos_ref, sin_ref, gb_ref, cg_ref, cv_ref,
    out_ref,
    packs, qn, qraw, qr, kup, vup, op, res, w, gbs, att, acc, mrun, lrun, dcol, docs, bias,
    sa, sp_buf, sm_buf, pfp, pfm, own, ra, rb, ra2, rb2, m4, nf, gv, hid, stat, stats,
    lsem, ssem, rsem,
):
    sp = lax.axis_index("sp")
    y = lax.axis_index("tp")
    c = lax.rem(sp, 2)
    k = lax.div(sp, 2)
    x = lax.rem(k, NX)
    z = lax.div(k, NX)

    def wrap(v, n):
        return lax.rem(v + n, n)

    def dev(zz, xx, cc, yy):
        return ((wrap(zz, NZ) * NX + wrap(xx, NX)) * 2 + cc, wrap(yy, NY))

    def chip(kk, cc):
        return (wrap(kk, NZ * NX) * 2 + cc, y)

    xp, xm = dev(z, x + 1, c, y), dev(z, x - 1, c, y)
    zp, zm = dev(z + 1, x, c, y), dev(z - 1, x, c, y)
    sib = dev(z, x, 1 - c, y)
    yp, ym, yy = dev(z, x, c, y + 1), dev(z, x, c, y - 1), dev(z, x, c, y + 2)
    nextc, prevc = chip(k + 1, c), chip(k - 1, c)
    nexto, prevo = chip(k + 1, 1 - c), chip(k - 1, 1 - c)

    local = []
    def fetch(src, dst):
        d = pltpu.make_async_copy(src, dst, lsem.at[len(local)])
        d.start()
        local.append(d)
        return d
    f_lat = fetch(lat_h, packs.at[0, :, pl.ds(0, 512)])
    mine = w.at[z, x, c]
    f_w = [
        fetch(gate_h, mine.at[:, pl.ds(DA, UNITS)]),
        fetch(value_h, mine.at[:, pl.ds(LA, UNITS)]),
        fetch(down_h.at[:, pl.ds(0, DA)], mine.at[:, pl.ds(0, DA)]),
        fetch(down_h.at[:, pl.ds(DA, UNITS - DA)], mine.at[:, pl.ds(LA + UNITS, UNITS - DA)]),
    ]
    f_qr = fetch(qr_h, qraw)
    f_kup = fetch(kup_h, kup)
    f_qn = fetch(qn_h, qn)
    f_vup = fetch(vup_h, vup)
    f_op = fetch(op_h, op)
    f_res = fetch(res_h, res)

    lane = lax.broadcasted_iota(jnp.int32, (ROWS, 128), 1)
    front = lax.rem(lane, ROPE) < ROPE // 2

    def turned(v):
        swapped = jnp.where(front, pltpu.roll(v, 128 - ROPE // 2, 1), pltpu.roll(v, ROPE // 2, 1))
        return v * cos_ref[...] + swapped * sin_ref[...]

    key = key_ref[...].astype(F32)
    packs[0, :, 512:640] = turned(jnp.concatenate([key, key], axis=0).T).astype(BF)
    docs[0] = jnp.broadcast_to(gb_ref[4:5, 0:ROWS], (8, ROWS))
    def doc_column(slot):
        return jnp.concatenate([docs[slot], jnp.zeros((120, ROWS), F32)], axis=0).T[:, 0:1]

    barrier = pltpu.get_barrier_semaphore()
    peers = (
        xp, xm, zp, zm, sib, yp, ym, yy, nextc, prevc, nexto, prevo,
        chip(k + 2, 1 - c), chip(k - 2, 1 - c),
    )
    for p in peers:
        pl.semaphore_signal(barrier, inc=1, device_id=p, device_id_type=MESH)
    pl.semaphore_wait(barrier, len(peers))

    sends = []
    zero_only = []
    names = {}

    def rid(name):
        return names.setdefault(name, len(names))

    def copy_to(src, dst, to, name):
        d = pltpu.make_async_remote_copy(
            src_ref=src, dst_ref=dst, send_sem=ssem.at[len(sends)],
            recv_sem=rsem.at[rid(name)], device_id=to, device_id_type=MESH,
        )
        sends.append(d)
        return d

    def copy_at(src, dst, to, name, at):
        return pltpu.make_async_remote_copy(
            src_ref=src, dst_ref=dst, send_sem=ssem.at[at],
            recv_sem=rsem.at[rid(name)], device_id=to, device_id_type=MESH,
        )

    def send(src, dst, to, name):
        copy_to(src, dst, to, name).start()

    def arrive(dst, name):
        pltpu.make_async_remote_copy(
            src_ref=dst, dst_ref=dst, send_sem=ssem.at[0],
            recv_sem=rsem.at[rid(name)], device_id=sib, device_id_type=MESH,
        ).wait_recv()

    def wa(dz, dx):
        return w.at[wrap(z + dz, NZ), wrap(x + dx, NX), c, :, pl.ds(0, LA)]

    def za(dz, cc, lo=0, n=NX):
        return w.at[wrap(z + dz, NZ), pl.ds(lo, n), cc, :, pl.ds(0, LA)]

    def wb(dz, lo=LA, n=LW - LA):
        return w.at[wrap(z + dz, NZ), x, c, :, pl.ds(lo, n)]

    def xb(dx, cc, lo=0, n=NZ):
        return w.at[pl.ds(lo, n), wrap(x + dx, NX), cc, :, pl.ds(LA, LW - LA)]

    BH = (LW - LA) // 2
    HZ = NZ // 2
    HX = NX // 2

    def same(ref, to, name):
        send(ref, ref, to, name)

    def a_start():
        same(wa(0, 0), xp, "a1m")
        same(wa(0, 0), xm, "a1p")

    def a_one():
        arrive(wa(0, 1), "a1p")
        same(wa(0, 1), xm, "a2p")

    def a_two():
        arrive(wa(0, -1), "a1m")
        arrive(wa(0, 2), "a2p")
        same(za(0, c), zp, "z1m")
        same(za(0, c), zm, "z1p")
        same(za(0, c), sib, "sz0")

    def a_step(s):
        arrive(za(-s, c), f"z{s}m")
        arrive(za(s, c), f"z{s}p")
        if s < 3:
            same(za(-s, c), zp, f"z{s + 1}m")
            same(za(s, c), zm, f"z{s + 1}p")
        else:
            same(za(-s, c, 0, HX), zp, "z4m")
            same(za(s, c, HX, HX), zm, "z4p")
        same(za(-s, c), sib, f"sz{s}m")
        same(za(s, c), sib, f"sz{s}p")

    def a_last():
        arrive(za(4, c, 0, HX), "z4m")
        arrive(za(4, c, HX, HX), "z4p")
        same(za(4, c), sib, "sz4")

    def a_done():
        arrive(za(0, 1 - c), "sz0")
        for s in (1, 2, 3):
            arrive(za(-s, 1 - c), f"sz{s}m")
            arrive(za(s, 1 - c), f"sz{s}p")
        arrive(za(4, 1 - c), "sz4")

    def b_start():
        same(wb(0), zp, "b1m")
        same(wb(0), zm, "b1p")

    def b_step(s):
        arrive(wb(-s), f"b{s}m")
        arrive(wb(s), f"b{s}p")
        if s < 3:
            same(wb(-s), zp, f"b{s + 1}m")
            same(wb(s), zm, f"b{s + 1}p")
        else:
            same(wb(-s, LA, BH), zp, "b4m")
            same(wb(s, LA + BH, BH), zm, "b4p")

    def b_turn():
        arrive(wb(4, LA, BH), "b4m")
        arrive(wb(4, LA + BH, BH), "b4p")
        same(xb(0, c), xp, "x1m")
        same(xb(0, c), xm, "x1p")
        same(xb(0, c), sib, "sx0")

    def b_cross():
        arrive(xb(-1, c), "x1m")
        arrive(xb(1, c), "x1p")
        same(xb(-1, c, 0, HZ), xp, "x2m")
        same(xb(1, c, HZ, HZ), xm, "x2p")
        same(xb(-1, c), sib, "sx1m")
        same(xb(1, c), sib, "sx1p")

    def b_last():
        arrive(xb(2, c, 0, HZ), "x2m")
        arrive(xb(2, c, HZ, HZ), "x2p")
        same(xb(2, c), sib, "sx2")

    def b_done():
        arrive(xb(0, 1 - c), "sx0")
        arrive(xb(-1, 1 - c), "sx1m")
        arrive(xb(1, 1 - c), "sx1p")
        arrive(xb(2, 1 - c), "sx2")

    QR = ROWS // NY

    def quarter(slot, dy, lo=0, n=QR):
        return packs.at[slot, pl.ds(pl.multiple_of(wrap(y + dy, NY) * QR + lo, 16), n)]

    def spread(slot, tag):
        def one():
            arrive(quarter(slot, 0), tag)
            same(quarter(slot, 0), yp, tag + "1m")
            same(quarter(slot, 0), ym, tag + "1p")

        def two():
            arrive(quarter(slot, -1), tag + "1m")
            same(quarter(slot, -1, 0, QR // 2), yp, tag + "2m")
            arrive(quarter(slot, 1), tag + "1p")
            same(quarter(slot, 1, QR // 2, QR // 2), ym, tag + "2p")

        def three():
            arrive(quarter(slot, 2, 0, QR // 2), tag + "2m")
            arrive(quarter(slot, 2, QR // 2, QR // 2), tag + "2p")

        return one, two, three

    f_lat.wait()
    send(quarter(0, 0), quarter(2, 0), nextc, "l2")
    send(docs.at[0], docs.at[2], nextc, "d2")
    for d in f_w:
        d.wait()
    a_start()
    b_start()

    @pl.when(c == 0)
    def _():
        copy_at(packs.at[0], packs.at[1], sib, "l1", S_ALT).start()
        copy_at(docs.at[0], docs.at[1], sib, "d1", S_ALT + 1).start()
        copy_at(docs.at[0], docs.at[3], nexto, "d3", S_ALT + 2).start()

    @pl.when(c == 1)
    def _():
        copy_at(docs.at[0], docs.at[1], nexto, "d1", S_ALT + 1).start()
        copy_at(docs.at[0], docs.at[3], chip(k + 2, 0), "d3", S_ALT + 2).start()

    send(gb_ref, gbs.at[y], yp, "gm")
    send(gb_ref, gbs.at[y], ym, "gp")
    send(gb_ref, gbs.at[y], yy, "g2")
    dcol[8 : 8 + ROWS, :] = jnp.broadcast_to(doc_column(0), (ROWS, 128))
    f_qr.wait()
    for t in range(4):
        v = turned(qraw[:, t * 128 : t * 128 + 128].astype(F32))
        qr[:, t * 256 : t * 256 + 128] = jnp.where(lane < ROPE, v, 0.0).astype(BF)
        qr[:, t * 256 + 128 : t * 256 + 256] = jnp.where(lane >= ROPE, v, 0.0).astype(BF)

    def attend(slot, back, kind, first=False, last=False):
        kdoc = jnp.where(sp >= back, docs[slot, 0:1, :], -1.0)
        ok = dcol[8 : 8 + ROWS, 0:1] == kdoc
        if kind == "diag":
            qi_pos = lax.broadcasted_iota(jnp.int32, (ROWS, ROWS), 0)
            ki_pos = lax.broadcasted_iota(jnp.int32, (ROWS, ROWS), 1)
            ok = ok & (ki_pos <= qi_pos)
        bias[...] = jnp.where(ok, 0.0, masked_score)
        ones = jnp.ones((ROWS, 128), BF)

        def body(group, carry):
            lat = packs[slot, :, 0:512]
            kr = packs[slot, :, 512:640]
            lanes, states, results = [], [], []
            for hh in range(GROUP):
                h = group * GROUP + hh
                lanes.append(pl.ds(pl.multiple_of(h * 128, 128), 128))
                if not first:
                    states.append((mrun[h], lrun[h], acc[h]))
            for hh in range(GROUP):
                if hh % 2 == 0:
                    both = pl.ds(pl.multiple_of((group * GROUP + hh) * 128, 256), 256)
                    k2 = dot(lat, kup[:, both]).astype(BF)
                    v2 = dot(lat, vup[:, both]).astype(BF)
                part = slice(hh % 2 * 128, hh % 2 * 128 + 128)
                kk = jnp.concatenate([k2[:, part], kr], axis=1)
                vv = jnp.concatenate([v2[:, part], ones], axis=1)
                q = jnp.concatenate([qn[:, lanes[hh]], qr[:, lanes[hh]]], axis=1)
                s = dot_nt(q, kk) + bias[...]
                mx = jnp.max(s, axis=1, keepdims=True)
                if first:
                    mnew = jnp.broadcast_to(mx, (ROWS, 128))
                else:
                    mnew = jnp.maximum(states[hh][0], mx)
                p = jnp.exp2((s - mnew[:, 0:1]) * SCALE2)
                o = dot(p.astype(BF), vv)
                o, total = o[:, 0:128], o[:, 128:256]
                if not first:
                    alpha = jnp.exp2((states[hh][0] - mnew) * SCALE2)
                    total = states[hh][1] * alpha + total
                    o = states[hh][2] * alpha + o
                results.append((mnew, total, o))
            for hh in range(GROUP):
                h = group * GROUP + hh
                mnew, total, o = results[hh]
                if last:
                    att[:, lanes[hh]] = (o / total).astype(BF)
                else:
                    mrun[h] = mnew
                    lrun[h] = total
                    acc[h] = o
            return carry

        lax.fori_loop(0, 8 // GROUP, body, 0)

    f_kup.wait()
    f_qn.wait()
    f_vup.wait()
    slot_two = spread(2, "l2")
    slot_three = spread(3, "l3")
    attend(0, 0, "diag", first=True)
    slot_two[0]()

    @pl.when(c == 1)
    def _():
        copy_at(quarter(2, 0), quarter(3, 0), nexto, "l3", S_ALT).start()

    a_one()
    b_step(1)
    slot_two[1]()
    b_step(2)
    slot_two[2]()

    @pl.when(c == 0)
    def _():
        copy_at(packs.at[2], packs.at[3], sib, "s3", S_ALT + 3).start()
        before = len(sends)
        slot_three[0]()
        for i in range(before, len(sends)):
            zero_only.append(i)
            sends[i] = None

    @pl.when(c == 1)
    def _():
        copy_at(packs.at[2], packs.at[1], sib, "l1", S_ALT + 3).start()

    b_step(3)
    arrive(docs.at[2], "d2")
    attend(2, 2, "full")
    a_two()
    b_turn()
    arrive(packs.at[1], "l1")
    arrive(docs.at[1], "d1")
    before = jnp.where(sp >= 1, doc_column(1)[ROWS - 8 : ROWS, :], -1.0)
    dcol[0:8, :] = jnp.broadcast_to(before, (8, 128))

    @pl.when(c == 0)
    def _():
        before = len(sends)
        slot_three[1]()
        for i in range(before, len(sends)):
            zero_only.append(i)
            sends[i] = None

    attend(1, 1, "full")
    arrive(docs.at[3], "d3")

    @pl.when(c == 0)
    def _():
        slot_three[2]()

    @pl.when(c == 1)
    def _():
        arrive(packs.at[3], "s3")

    attend(3, 3, "far", last=True)
    a_step(1)

    def shared_sum(chunk, tag, ra, rb, pump_one, pump_two):
        f = chunk(wrap(y + 2, NY))
        sa[...] = f.astype(BF)
        send(sa.at[pl.ds(0, HALF)], ra.at[0], yp, tag + "am")
        send(sa.at[pl.ds(HALF, HALF)], ra.at[1], ym, tag + "ap")
        f = chunk(wrap(y + 1, NY))
        pfp[...] = f[:HALF]
        sp_buf[pl.ds(HALF, HALF), :] = f[HALF:].astype(BF)
        send(sp_buf.at[pl.ds(HALF, HALF)], rb.at[0, pl.ds(HALF, HALF)], yp, tag + "bm1")
        f = chunk(wrap(y - 1, NY))
        pfm[...] = f[HALF:]
        sm_buf[pl.ds(0, HALF), :] = f[:HALF].astype(BF)
        send(sm_buf.at[pl.ds(0, HALF)], rb.at[1, pl.ds(0, HALF)], ym, tag + "bp0")
        own[...] = chunk(y)
        pump_one()
        arrive(ra.at[0], tag + "am")
        sp_buf[pl.ds(0, HALF), :] = (pfp[...] + ra[0].astype(F32)).astype(BF)
        send(sp_buf.at[pl.ds(0, HALF)], rb.at[0, pl.ds(0, HALF)], yp, tag + "bm0")
        arrive(ra.at[1], tag + "ap")
        sm_buf[pl.ds(HALF, HALF), :] = (pfm[...] + ra[1].astype(F32)).astype(BF)
        send(sm_buf.at[pl.ds(HALF, HALF)], rb.at[1, pl.ds(HALF, HALF)], ym, tag + "bp1")
        pump_two()
        arrive(rb.at[0, pl.ds(HALF, HALF)], tag + "bm1")
        arrive(rb.at[1, pl.ds(0, HALF)], tag + "bp0")
        arrive(rb.at[0, pl.ds(0, HALF)], tag + "bm0")
        arrive(rb.at[1, pl.ds(HALF, HALF)], tag + "bp1")
        return own[...] + rb[0].astype(F32) + rb[1].astype(F32)

    def settle(ds):
        for d in ds:
            d.wait_send()

    f_op.wait()
    f_res.wait()

    def head_share(t):
        return dot(att[...], op[:, pl.ds(pl.multiple_of(t * CH, CH), CH)])

    mark = len(sends)
    total_one = shared_sum(head_share, "p", ra, rb, lambda: None, lambda: a_step(2))
    m4[y] = (residual_scale * res[...].astype(F32) + total_one).astype(BF)

    def piece(dy, lo):
        return m4.at[wrap(y + dy, NY), pl.ds(lo, HALF)]

    same(piece(0, 0), yp, "m1m0")
    same(piece(0, HALF), ym, "m1p1")
    same(piece(0, HALF), yp, "m1m1")
    same(piece(0, 0), ym, "m1p0")
    b_cross()
    arrive(piece(-1, 0), "m1m0")
    same(piece(-1, 0), yp, "m2m")
    arrive(piece(1, HALF), "m1p1")
    same(piece(1, HALF), ym, "m2p")
    arrive(gbs.at[wrap(y - 1, NY)], "gm")
    arrive(gbs.at[wrap(y + 1, NY)], "gp")
    arrive(gbs.at[wrap(y + 2, NY)], "g2")
    gbs[y] = gb_ref[...]
    a_step(3)
    arrive(piece(-1, HALF), "m1m1")
    arrive(piece(1, 0), "m1p0")
    arrive(piece(2, 0), "m2m")
    arrive(piece(2, HALF), "m2p")

    def norm_rows(i, carry):
        rows = pl.ds(pl.multiple_of(i * 32, 32), 32)
        parts = [m4[t, rows, :].astype(F32) for t in range(NY)]
        s = sum(jnp.sum(v, axis=1, keepdims=True) for v in parts) / D
        q = sum(jnp.sum(v * v, axis=1, keepdims=True) for v in parts) / D
        r = lax.rsqrt(q - s * s + norm_eps)
        for t in range(NY):
            nf[rows, t * CH : (t + 1) * CH] = (
                (parts[t] - s) * r * gbs[t, 0:1, :] + gbs[t, 1:2, :]
            ).astype(BF)
        return carry

    lax.fori_loop(0, ROWS // 32, norm_rows, 0)
    b_last()
    a_last()
    b_done()
    a_done()

    def up(j, carry):
        lanes = pl.ds(pl.multiple_of(DA + j * 256, 128), 256)
        f = dot(nf[...], w[:, :, :, :, lanes].reshape(D, 256))
        gv[8 : 8 + ROWS, pl.ds(pl.multiple_of(j * 256, 256), 256)] = f
        return carry

    lax.fori_loop(0, 2 * UNITS // 256, up, 0)
    tail = pl.ds(ROWS, 8)

    to_sib = copy_to(gv.at[tail], stat.at[0], sib, "t")
    to_next = pltpu.make_async_remote_copy(
        src_ref=gv.at[tail], dst_ref=stat.at[0], send_sem=ssem.at[len(sends) - 1],
        recv_sem=rsem.at[rid("t")], device_id=nexto, device_id_type=MESH,
    )

    @pl.when(c == 0)
    def _():
        to_sib.start()

    @pl.when(c == 1)
    def _():
        to_next.start()

    def conv_block(r0):
        here = dcol[8 + r0 : 8 + r0 + 128, :]
        one = (dcol[7 + r0 : 7 + r0 + 128, :] == here).astype(F32)
        two = (dcol[6 + r0 : 6 + r0 + 128, :] == here).astype(F32)

        def cols(j, carry):
            def mix(taps, base):
                lanes = pl.ds(pl.multiple_of(base + j * 128, 128), 128)
                a0 = gv[6 + r0 : 6 + r0 + 128, lanes]
                a1 = gv[7 + r0 : 7 + r0 + 128, lanes]
                a2 = gv[8 + r0 : 8 + r0 + 128, lanes]
                t = taps[:, pl.ds(pl.multiple_of(j * 128, 128), 128)].astype(F32)
                return t[0:1] * a0 * two + t[1:2] * a1 * one + t[2:3] * a2

            g = mix(cg_ref, 0)
            v = mix(cv_ref, UNITS)
            act = 0.5 * g * (1.0 + jnp.tanh(0.7978845608028654 * (g + 0.044715 * (g * g * g))))
            hid[r0 : r0 + 128, pl.ds(pl.multiple_of(j * 128, 128), 128)] = (v * act).astype(BF)
            return carry

        lax.fori_loop(0, UNITS // 128, cols, 0)

    conv_block(256)
    conv_block(128)
    arrive(stat.at[0], "t")
    gv[0:8, :] = jnp.where(sp >= 1, stat[0], 0.0)
    conv_block(0)

    def unit_share(t):
        rows = pl.ds(2 * t, 2)
        da = w[rows, :, :, :, 0:DA].reshape(CH, DA)
        db = w[rows, :, :, :, LA + UNITS : LW].reshape(CH, UNITS - DA)
        return dot_nt(hid[:, 0:DA], da) + dot_nt(hid[:, DA:UNITS], db)

    settle(sends[mark : mark + 6])
    total_two = shared_sum(unit_share, "u", ra2, rb2, lambda: None, lambda: None)
    mixed = (
        residual_scale * nf[:, pl.ds(pl.multiple_of(y * CH, CH), CH)].astype(F32) + total_two
    )
    own[...] = mixed
    s = jnp.sum(mixed, axis=1, keepdims=True)
    q = jnp.sum(mixed * mixed, axis=1, keepdims=True)
    both = jnp.where(lane == 0, s, jnp.where(lane == 1, q, 0.0))
    stats[y] = both.T[0:8, :]
    same(stats.at[y], yp, "qm")
    same(stats.at[y], ym, "qp")
    same(stats.at[y], yy, "q2")
    arrive(stats.at[wrap(y - 1, NY)], "qm")
    arrive(stats.at[wrap(y + 1, NY)], "qp")
    arrive(stats.at[wrap(y + 2, NY)], "q2")
    tot = (stats[0] + stats[1]) + (stats[2] + stats[3])
    back = jnp.concatenate([tot, jnp.zeros((120, ROWS), F32)], axis=0).T
    s = back[:, 0:1] / D
    q = back[:, 1:2] / D
    r = lax.rsqrt(q - s * s + norm_eps)
    out_ref[...] = ((own[...] - s) * r * gbs[y, 2:3, :] + gbs[y, 3:4, :]).astype(BF)
    settle(d for d in sends[:mark] if d is not None)
    settle(sends[mark + 6 :])
    copy_at(docs.at[0], docs.at[1], sib, "d1", S_ALT + 1).wait_send()
    copy_at(docs.at[0], docs.at[3], sib, "d3", S_ALT + 2).wait_send()
    copy_at(packs.at[2], packs.at[3], sib, "s3", S_ALT + 3).wait_send()

    @pl.when(c == 0)
    def _():
        copy_at(packs.at[0], packs.at[1], sib, "l1", S_ALT).wait_send()
        for i, at in enumerate(zero_only):
            part = quarter(3, 0, 0, QR if i < 2 else QR // 2)
            copy_at(part, part, yp, "l3", at).wait_send()

    @pl.when(c == 1)
    def _():
        copy_at(quarter(2, 0), quarter(3, 0), nexto, "l3", S_ALT).wait_send()


def tables(positions):
    frequencies = 1.0 / rope_base_freq ** (jnp.arange(0, ROPE, 2, dtype=jnp.float32) / ROPE)
    angles = positions.astype(jnp.float32)[:, None] * jnp.tile(frequencies, 4)[None, :]
    sign = jnp.where(jnp.arange(128) % ROPE < ROPE // 2, -1.0, 1.0).astype(jnp.float32)
    return (jnp.cos(angles), jnp.sin(angles) * sign[None, :])


def local(
    residual, query_nope, query_rope, latent, rope_key, doc_ids, key_up, value_up, out_proj,
    norm1_gain, norm1_bias, ffn_gate, ffn_value, conv_gate, conv_value, ffn_down,
    norm2_gain, norm2_bias,
):
    rows = latent.shape[0]
    positions = lax.axis_index("sp") * rows + jnp.arange(rows, dtype=jnp.int32)
    cosine, sine = tables(positions)
    doc = jnp.pad(doc_ids.astype(BF), (0, CH - rows))
    none = jnp.zeros((3 * CH,), BF)
    vectors = jnp.concatenate([norm1_gain, norm1_bias, norm2_gain, norm2_bias, doc, none])
    vectors = vectors.astype(F32).reshape(8, CH)

    anyspec = pl.BlockSpec(memory_space=pl.ANY)
    vspec = pl.BlockSpec(memory_space=pltpu.VMEM)
    V = pltpu.VMEM
    return pl.pallas_call(
        layer_kernel,
        out_shape=jax.ShapeDtypeStruct((rows, CH), BF),
        in_specs=[anyspec] * 10 + [vspec] * 6,
        out_specs=vspec,
        scratch_shapes=[
            V((4, ROWS, PACKW), BF),
            V((ROWS, 1024), BF),
            V((ROWS, CH), BF),
            V((ROWS, 1024), BF),
            V((512, 1024), BF),
            V((512, 1024), BF),
            V((1024, D), BF),
            V((ROWS, CH), BF),
            V((NZ, NX, 2, 32, LW), BF),
            V((NY, 8, CH), F32),
            V((ROWS, 1024), BF),
            V((8, ROWS, 128), F32),
            V((8, ROWS, 128), F32),
            V((8, ROWS, 128), F32),
            V((8 + ROWS, 128), F32),
            V((4, 8, ROWS), F32),
            V((ROWS, ROWS), F32),
            V((ROWS, CH), BF),
            V((ROWS, CH), BF),
            V((ROWS, CH), BF),
            V((HALF, CH), F32),
            V((HALF, CH), F32),
            V((ROWS, CH), F32),
            V((2, HALF, CH), BF),
            V((2, ROWS, CH), BF),
            V((2, HALF, CH), BF),
            V((2, ROWS, CH), BF),
            V((NY, ROWS, CH), BF),
            V((ROWS, D), BF),
            V((8 + ROWS, 2 * UNITS), F32),
            V((ROWS, UNITS), BF),
            V((1, 8, 2 * UNITS), F32),
            V((NY, 8, ROWS), F32),
            pltpu.SemaphoreType.DMA((11,)),
            pltpu.SemaphoreType.DMA((N_SEND,)),
            pltpu.SemaphoreType.DMA((N_RECV,)),
        ],
        compiler_params=pltpu.CompilerParams(
            collective_id=0, has_side_effects=True, vmem_limit_bytes=60 * 1024 * 1024
        ),
    )(
        latent, query_nope, query_rope, key_up, value_up, out_proj, residual,
        ffn_gate, ffn_value, ffn_down.T, rope_key.T, cosine, sine,
        vectors, conv_gate, conv_value,
    )


def solution(mesh):
    placed = (
        P("sp", "tp"),
        P("sp", "tp"),
        P("sp", "tp"),
        P("sp", None),
        P("sp", None),
        P("sp"),
        P(None, "tp"),
        P(None, "tp"),
        P("tp", None),
        P("tp"),
        P("tp"),
        P("sp", "tp"),
        P("sp", "tp"),
        P(None, "tp"),
        P(None, "tp"),
        P("tp", "sp"),
        P("tp"),
        P("tp"),
    )
    return jax.shard_map(
        local, mesh=mesh, in_specs=placed, out_specs=P("sp", "tp"), check_vma=False
    )
```

```python
import jax
import jax.numpy as jnp
import numpy as np
from jax import lax
from jax.experimental import pallas as pl
from jax.experimental.pallas import tpu as pltpu
from jax.sharding import PartitionSpec as P

D = 2048
NOPE = 128
ROPE = 64
VDIM = 128
CONV = 3
REACH = 3

norm_eps = 1e-05
residual_scale = 8.0**0.25
rope_base_freq = 10000.0
masked_score = -1e30
SCALE2 = (NOPE + ROPE) ** (-0.5) * 1.4426950408889634

NX, NZ, NY = 4, 8, 4
ROWS = 384
HALF = ROWS // 2
CH = 512
UNITS = 1408
DA = 256
LA = DA + UNITS
LW = 3 * UNITS
PACKW = 640
GROUP = 4
N_SEND = 128
N_RECV = 128
S_ALT = N_SEND - 4
MESH = pl.DeviceIdType.MESH
BF = jnp.bfloat16
F32 = jnp.float32


def dot(a, b):
    return jnp.dot(a, b, preferred_element_type=F32)


def dot_nt(a, b):
    return lax.dot_general(a, b, (((1,), (1,)), ((), ())), preferred_element_type=F32)


def layer_kernel(
    lat_h, qn_h, qr_h, kup_h, vup_h, op_h, res_h, gate_h, value_h, down_h,
    key_h, g1_h, b1_h, g2_h, b2_h, doc_h, cg_h, cv_h, freq_h,
    out_ref,
    key_ref, v0, v1, v2, v3, doc_ref, cg_ref, cv_ref, freq_ref, gb_ref, cos_ref, sin_ref,
    packs, qn, qraw, qr, kup, vup, op, res, w, gbs, att, acc, mrun, lrun, dcol, docs, bias,
    sa, sp_buf, sm_buf, pfp, pfm, own, ra, rb, ra2, rb2, m4, nf, gv, hid, stat, stats,
    lsem, ssem, rsem,
):
    sp = lax.axis_index("sp")
    y = lax.axis_index("tp")
    c = lax.rem(sp, 2)
    k = lax.div(sp, 2)
    x = lax.rem(k, NX)
    z = lax.div(k, NX)

    def wrap(v, n):
        return lax.rem(v + n, n)

    def dev(zz, xx, cc, yy):
        return ((wrap(zz, NZ) * NX + wrap(xx, NX)) * 2 + cc, wrap(yy, NY))

    def chip(kk, cc):
        return (wrap(kk, NZ * NX) * 2 + cc, y)

    xp, xm = dev(z, x + 1, c, y), dev(z, x - 1, c, y)
    zp, zm = dev(z + 1, x, c, y), dev(z - 1, x, c, y)
    sib = dev(z, x, 1 - c, y)
    yp, ym, yy = dev(z, x, c, y + 1), dev(z, x, c, y - 1), dev(z, x, c, y + 2)
    nextc, prevc = chip(k + 1, c), chip(k - 1, c)
    nexto, prevo = chip(k + 1, 1 - c), chip(k - 1, 1 - c)

    local = []
    def fetch(src, dst):
        d = pltpu.make_async_copy(src, dst, lsem.at[len(local)])
        d.start()
        local.append(d)
        return d
    f_small = [
        fetch(key_h, key_ref),
        fetch(freq_h, freq_ref),
        fetch(doc_h, doc_ref),
        fetch(g1_h, v0),
        fetch(b1_h, v1),
        fetch(g2_h, v2),
        fetch(b2_h, v3),
    ]
    f_lat = fetch(lat_h, packs.at[0, :, pl.ds(0, 512)])
    mine = w.at[z, x, c]
    f_w = [
        fetch(gate_h, mine.at[:, pl.ds(DA, UNITS)]),
        fetch(value_h, mine.at[:, pl.ds(LA, UNITS)]),
        fetch(down_h.at[:, pl.ds(0, DA)], mine.at[:, pl.ds(0, DA)]),
        fetch(down_h.at[:, pl.ds(DA, UNITS - DA)], mine.at[:, pl.ds(LA + UNITS, UNITS - DA)]),
    ]
    f_qr = fetch(qr_h, qraw)
    f_kup = fetch(kup_h, kup)
    f_qn = fetch(qn_h, qn)
    f_vup = fetch(vup_h, vup)
    f_taps = [fetch(cg_h, cg_ref), fetch(cv_h, cv_ref)]
    f_op = fetch(op_h, op)
    f_res = fetch(res_h, res)

    barrier = pltpu.get_barrier_semaphore()
    peers = (
        xp, xm, zp, zm, sib, yp, ym, yy, nextc, prevc, nexto, prevo,
        chip(k + 2, 1 - c), chip(k - 2, 1 - c),
    )
    for p in peers:
        pl.semaphore_signal(barrier, inc=1, device_id=p, device_id_type=MESH)
    lane = lax.broadcasted_iota(jnp.int32, (ROWS, 128), 1)
    front = lax.rem(lane, ROPE) < ROPE // 2

    def turned(v):
        swapped = jnp.where(front, pltpu.roll(v, 128 - ROPE // 2, 1), pltpu.roll(v, ROPE // 2, 1))
        return v * cos_ref[...] + swapped * sin_ref[...]

    for d in f_small:
        d.wait()
    place = lax.broadcasted_iota(jnp.int32, (ROWS, 128), 0) + sp * ROWS
    angle = place.astype(F32) * freq_ref[0:1, :]
    cos_ref[...] = jnp.cos(angle)
    sin_ref[...] = jnp.where(front, -1.0, 1.0) * jnp.sin(angle)
    key = key_ref[...].astype(F32)
    packs[0, :, 512:640] = turned(jnp.concatenate([key, key], axis=0).T).astype(BF)
    docs[0] = jnp.broadcast_to(doc_ref[...].astype(F32).reshape(1, ROWS), (8, ROWS))
    gb_ref[...] = jnp.concatenate(
        [v[...].astype(F32).reshape(1, CH) for v in (v0, v1, v2, v3)] + [jnp.zeros((4, CH), F32)], axis=0
    )
    def doc_column(slot):
        return jnp.concatenate([docs[slot], jnp.zeros((120, ROWS), F32)], axis=0).T[:, 0:1]

    pl.semaphore_wait(barrier, len(peers))

    sends = []
    zero_only = []
    names = {}

    def rid(name):
        return names.setdefault(name, len(names))

    def copy_to(src, dst, to, name):
        d = pltpu.make_async_remote_copy(
            src_ref=src, dst_ref=dst, send_sem=ssem.at[len(sends)],
            recv_sem=rsem.at[rid(name)], device_id=to, device_id_type=MESH,
        )
        sends.append(d)
        return d

    def copy_at(src, dst, to, name, at):
        return pltpu.make_async_remote_copy(
            src_ref=src, dst_ref=dst, send_sem=ssem.at[at],
            recv_sem=rsem.at[rid(name)], device_id=to, device_id_type=MESH,
        )

    def send(src, dst, to, name):
        copy_to(src, dst, to, name).start()

    def arrive(dst, name):
        pltpu.make_async_remote_copy(
            src_ref=dst, dst_ref=dst, send_sem=ssem.at[0],
            recv_sem=rsem.at[rid(name)], device_id=sib, device_id_type=MESH,
        ).wait_recv()

    def wa(dz, dx):
        return w.at[wrap(z + dz, NZ), wrap(x + dx, NX), c, :, pl.ds(0, LA)]

    def za(dz, cc, lo=0, n=NX):
        return w.at[wrap(z + dz, NZ), pl.ds(lo, n), cc, :, pl.ds(0, LA)]

    def wb(dz, lo=LA, n=LW - LA):
        return w.at[wrap(z + dz, NZ), x, c, :, pl.ds(lo, n)]

    def xb(dx, cc, lo=0, n=NZ):
        return w.at[pl.ds(lo, n), wrap(x + dx, NX), cc, :, pl.ds(LA, LW - LA)]

    BH = (LW - LA) // 2
    HX = NX // 2

    def bp(dz, dx):
        return w.at[wrap(z + dz, NZ), wrap(x + dx, NX), c, :, pl.ds(LA, LW - LA)]

    def same(ref, to, name):
        send(ref, ref, to, name)

    def a_start():
        same(wa(0, 0), xp, "a1m")
        same(wa(0, 0), xm, "a1p")

    def za_piece(dx):
        same(wa(0, dx), zp, f"z1m{dx}")
        same(wa(0, dx), zm, f"z1p{dx}")

    def a_one():
        arrive(wa(0, 1), "a1p")
        same(wa(0, 1), xm, "a2p")
        za_piece(1)

    def a_two():
        arrive(wa(0, -1), "a1m")
        za_piece(-1)
        arrive(wa(0, 2), "a2p")
        za_piece(2)
        same(za(0, c), sib, "sz0")

    def a_step(s):
        if s == 1:
            for dx in (0, 1, -1, 2):
                arrive(wa(-1, dx), f"z1m{dx}")
                arrive(wa(1, dx), f"z1p{dx}")
        else:
            arrive(za(-s, c), f"z{s}m")
            arrive(za(s, c), f"z{s}p")
        if s < 3:
            same(za(-s, c), zp, f"z{s + 1}m")
            same(za(s, c), zm, f"z{s + 1}p")
        else:
            same(za(-s, c, 0, HX), zp, "z4m")
            same(za(s, c, HX, HX), zm, "z4p")
        same(za(-s, c), sib, f"sz{s}m")
        same(za(s, c), sib, f"sz{s}p")

    def a_last():
        arrive(za(4, c, 0, HX), "z4m")
        arrive(za(4, c, HX, HX), "z4p")
        same(za(4, c), sib, "sz4")

    def a_done():
        arrive(za(0, 1 - c), "sz0")
        for s in (1, 2, 3):
            arrive(za(-s, 1 - c), f"sz{s}m")
            arrive(za(s, 1 - c), f"sz{s}p")
        arrive(za(4, 1 - c), "sz4")

    def bx_piece(dz):
        same(bp(dz, 0), xp, f"x1m{dz}")
        same(bp(dz, 0), xm, f"x1p{dz}")

    def b_start():
        same(wb(0), zp, "b1m")
        same(wb(0), zm, "b1p")

    def b_step(s):
        arrive(wb(-s), f"b{s}m")
        arrive(wb(s), f"b{s}p")
        if s < 3:
            same(wb(-s), zp, f"b{s + 1}m")
            same(wb(s), zm, f"b{s + 1}p")
        else:
            same(wb(-s, LA, BH), zp, "b4m")
            same(wb(s, LA + BH, BH), zm, "b4p")
        bx_piece(-s)
        bx_piece(s)

    def b_turn():
        arrive(wb(4, LA, BH), "b4m")
        arrive(wb(4, LA + BH, BH), "b4p")
        bx_piece(4)
        same(xb(0, c), sib, "sx0")

    DOWN = (-1, -2, -3, 4)

    def b_cross(i):
        up, down = i, DOWN[i]
        arrive(bp(up, -1), f"x1m{up}")
        same(bp(up, -1), xp, f"x2m{up}")
        arrive(bp(down, 1), f"x1p{down}")
        same(bp(down, 1), xm, f"x2p{down}")
        same(bp(up, -1), sib, "sx1m")
        same(bp(down, 1), sib, "sx1p")

    def b_collect(i):
        up, down = i, DOWN[i]
        arrive(bp(down, -1), f"x1m{down}")
        arrive(bp(up, 1), f"x1p{up}")
        same(bp(down, -1), sib, "sx1m")
        same(bp(up, 1), sib, "sx1p")

    def b_last(i):
        up, down = i, DOWN[i]
        arrive(bp(up, 2), f"x2m{up}")
        arrive(bp(down, 2), f"x2p{down}")
        same(bp(up, 2), sib, "sx2")
        same(bp(down, 2), sib, "sx2")

    def b_done():
        arrive(xb(0, 1 - c), "sx0")
        arrive(xb(-1, 1 - c), "sx1m")
        arrive(xb(1, 1 - c), "sx1p")
        arrive(xb(2, 1 - c), "sx2")

    QR = ROWS // NY

    def quarter(slot, dy, lo=0, n=QR):
        return packs.at[slot, pl.ds(pl.multiple_of(wrap(y + dy, NY) * QR + lo, 16), n)]

    def spread(slot, tag):
        def one():
            arrive(quarter(slot, 0), tag)
            same(quarter(slot, 0), yp, tag + "1m")
            same(quarter(slot, 0), ym, tag + "1p")

        def two():
            arrive(quarter(slot, -1), tag + "1m")
            same(quarter(slot, -1, 0, QR // 2), yp, tag + "2m")
            arrive(quarter(slot, 1), tag + "1p")
            same(quarter(slot, 1, QR // 2, QR // 2), ym, tag + "2p")

        def three():
            arrive(quarter(slot, 2, 0, QR // 2), tag + "2m")
            arrive(quarter(slot, 2, QR // 2, QR // 2), tag + "2p")

        return one, two, three

    f_lat.wait()
    send(quarter(0, 0), quarter(2, 0), nextc, "l2")
    send(docs.at[0], docs.at[2], nextc, "d2")
    for d in f_w:
        d.wait()
    a_start()
    b_start()
    bx_piece(0)
    za_piece(0)

    @pl.when(c == 0)
    def _():
        copy_at(packs.at[0], packs.at[1], sib, "l1", S_ALT).start()
        copy_at(docs.at[0], docs.at[1], sib, "d1", S_ALT + 1).start()
        copy_at(docs.at[0], docs.at[3], nexto, "d3", S_ALT + 2).start()

    @pl.when(c == 1)
    def _():
        copy_at(docs.at[0], docs.at[1], nexto, "d1", S_ALT + 1).start()
        copy_at(docs.at[0], docs.at[3], chip(k + 2, 0), "d3", S_ALT + 2).start()

    send(gb_ref, gbs.at[y], yp, "gm")
    send(gb_ref, gbs.at[y], ym, "gp")
    send(gb_ref, gbs.at[y], yy, "g2")
    dcol[8 : 8 + ROWS, :] = jnp.broadcast_to(doc_column(0), (ROWS, 128))
    f_qr.wait()
    for t in range(4):
        v = turned(qraw[:, t * 128 : t * 128 + 128].astype(F32))
        qr[:, t * 256 : t * 256 + 128] = jnp.where(lane < ROPE, v, 0.0).astype(BF)
        qr[:, t * 256 + 128 : t * 256 + 256] = jnp.where(lane >= ROPE, v, 0.0).astype(BF)

    def attend(slot, back, kind, first=False, last=False):
        kdoc = jnp.where(sp >= back, docs[slot, 0:1, :], -1.0)
        ok = dcol[8 : 8 + ROWS, 0:1] == kdoc
        if kind == "diag":
            qi_pos = lax.broadcasted_iota(jnp.int32, (ROWS, ROWS), 0)
            ki_pos = lax.broadcasted_iota(jnp.int32, (ROWS, ROWS), 1)
            ok = ok & (ki_pos <= qi_pos)
        bias[...] = jnp.where(ok, 0.0, masked_score)
        ones = jnp.ones((ROWS, 128), BF)

        def body(group, carry):
            lat = packs[slot, :, 0:512]
            kr = packs[slot, :, 512:640]
            lanes, states, results = [], [], []
            for hh in range(GROUP):
                h = group * GROUP + hh
                lanes.append(pl.ds(pl.multiple_of(h * 128, 128), 128))
                if not first:
                    states.append((mrun[h], lrun[h], acc[h]))
            for hh in range(GROUP):
                if hh % 2 == 0:
                    both = pl.ds(pl.multiple_of((group * GROUP + hh) * 128, 256), 256)
                    k2 = dot(lat, kup[:, both]).astype(BF)
                    v2 = dot(lat, vup[:, both]).astype(BF)
                part = slice(hh % 2 * 128, hh % 2 * 128 + 128)
                kk = jnp.concatenate([k2[:, part], kr], axis=1)
                vv = jnp.concatenate([v2[:, part], ones], axis=1)
                q = jnp.concatenate([qn[:, lanes[hh]], qr[:, lanes[hh]]], axis=1)
                s = dot_nt(q, kk) + bias[...]
                mx = jnp.max(s, axis=1, keepdims=True)
                if first:
                    mnew = jnp.broadcast_to(mx, (ROWS, 128))
                else:
                    mnew = jnp.maximum(states[hh][0], mx)
                p = jnp.exp2((s - mnew[:, 0:1]) * SCALE2)
                o = dot(p.astype(BF), vv)
                o, total = o[:, 0:128], o[:, 128:256]
                if not first:
                    alpha = jnp.exp2((states[hh][0] - mnew) * SCALE2)
                    total = states[hh][1] * alpha + total
                    o = states[hh][2] * alpha + o
                results.append((mnew, total, o))
            for hh in range(GROUP):
                h = group * GROUP + hh
                mnew, total, o = results[hh]
                if last:
                    att[:, lanes[hh]] = (o / total).astype(BF)
                else:
                    mrun[h] = mnew
                    lrun[h] = total
                    acc[h] = o
            return carry

        lax.fori_loop(0, 8 // GROUP, body, 0)

    f_kup.wait()
    f_qn.wait()
    f_vup.wait()
    slot_two = spread(2, "l2")
    slot_three = spread(3, "l3")
    attend(0, 0, "diag", first=True)
    slot_two[0]()

    @pl.when(c == 1)
    def _():
        copy_at(quarter(2, 0), quarter(3, 0), nexto, "l3", S_ALT).start()

    a_one()
    b_step(1)
    slot_two[1]()
    a_two()
    slot_two[2]()

    @pl.when(c == 0)
    def _():
        copy_at(packs.at[2], packs.at[3], sib, "s3", S_ALT + 3).start()
        before = len(sends)
        slot_three[0]()
        for i in range(before, len(sends)):
            zero_only.append(i)
            sends[i] = None

    @pl.when(c == 1)
    def _():
        copy_at(packs.at[2], packs.at[1], sib, "l1", S_ALT + 3).start()

    arrive(docs.at[2], "d2")
    attend(2, 2, "full")
    b_step(2)
    b_cross(0)

    @pl.when(c == 0)
    def _():
        before = len(sends)
        slot_three[1]()
        for i in range(before, len(sends)):
            zero_only.append(i)
            sends[i] = None

    arrive(packs.at[1], "l1")
    arrive(docs.at[1], "d1")
    before = jnp.where(sp >= 1, doc_column(1)[ROWS - 8 : ROWS, :], -1.0)
    dcol[0:8, :] = jnp.broadcast_to(before, (8, 128))
    attend(1, 1, "full")
    b_step(3)
    a_step(1)
    arrive(docs.at[3], "d3")

    @pl.when(c == 0)
    def _():
        slot_three[2]()

    @pl.when(c == 1)
    def _():
        arrive(packs.at[3], "s3")

    attend(3, 3, "far", last=True)

    def shared_sum(chunk, tag, ra, rb, pump_one, pump_two):
        f = chunk(wrap(y + 2, NY))
        sa[...] = f.astype(BF)
        send(sa.at[pl.ds(0, HALF)], ra.at[0], yp, tag + "am")
        send(sa.at[pl.ds(HALF, HALF)], ra.at[1], ym, tag + "ap")
        f = chunk(wrap(y + 1, NY))
        pfp[...] = f[:HALF]
        sp_buf[pl.ds(HALF, HALF), :] = f[HALF:].astype(BF)
        send(sp_buf.at[pl.ds(HALF, HALF)], rb.at[0, pl.ds(HALF, HALF)], yp, tag + "bm1")
        f = chunk(wrap(y - 1, NY))
        pfm[...] = f[HALF:]
        sm_buf[pl.ds(0, HALF), :] = f[:HALF].astype(BF)
        send(sm_buf.at[pl.ds(0, HALF)], rb.at[1, pl.ds(0, HALF)], ym, tag + "bp0")
        own[...] = chunk(y)
        pump_one()
        arrive(ra.at[0], tag + "am")
        sp_buf[pl.ds(0, HALF), :] = (pfp[...] + ra[0].astype(F32)).astype(BF)
        send(sp_buf.at[pl.ds(0, HALF)], rb.at[0, pl.ds(0, HALF)], yp, tag + "bm0")
        arrive(ra.at[1], tag + "ap")
        sm_buf[pl.ds(HALF, HALF), :] = (pfm[...] + ra[1].astype(F32)).astype(BF)
        send(sm_buf.at[pl.ds(HALF, HALF)], rb.at[1, pl.ds(HALF, HALF)], ym, tag + "bp1")
        pump_two()
        arrive(rb.at[0, pl.ds(HALF, HALF)], tag + "bm1")
        arrive(rb.at[1, pl.ds(0, HALF)], tag + "bp0")
        arrive(rb.at[0, pl.ds(0, HALF)], tag + "bm0")
        arrive(rb.at[1, pl.ds(HALF, HALF)], tag + "bp1")
        return own[...] + rb[0].astype(F32) + rb[1].astype(F32)

    def settle(ds):
        for d in ds:
            d.wait_send()

    f_op.wait()
    f_res.wait()

    def head_share(t):
        return dot(att[...], op[:, pl.ds(pl.multiple_of(t * CH, CH), CH)])

    mark = len(sends)

    def pump_early():
        b_turn()
        b_cross(1)
        b_cross(2)

    def pump_late():
        a_step(2)
        b_cross(3)
        for i in range(4):
            b_collect(i)

    total_one = shared_sum(head_share, "p", ra, rb, pump_early, pump_late)
    m4[y] = (residual_scale * res[...].astype(F32) + total_one).astype(BF)

    def piece(dy, lo):
        return m4.at[wrap(y + dy, NY), pl.ds(lo, HALF)]

    same(piece(0, 0), yp, "m1m0")
    same(piece(0, HALF), ym, "m1p1")
    same(piece(0, HALF), yp, "m1m1")
    same(piece(0, 0), ym, "m1p0")
    arrive(piece(-1, 0), "m1m0")
    same(piece(-1, 0), yp, "m2m")
    arrive(piece(1, HALF), "m1p1")
    same(piece(1, HALF), ym, "m2p")
    arrive(gbs.at[wrap(y - 1, NY)], "gm")
    arrive(gbs.at[wrap(y + 1, NY)], "gp")
    arrive(gbs.at[wrap(y + 2, NY)], "g2")
    gbs[y] = gb_ref[...]
    a_step(3)
    arrive(piece(-1, HALF), "m1m1")
    arrive(piece(1, 0), "m1p0")
    for i in range(4):
        b_last(i)
    arrive(piece(2, 0), "m2m")
    arrive(piece(2, HALF), "m2p")

    def norm_rows(i, carry):
        rows = pl.ds(pl.multiple_of(i * 32, 32), 32)
        parts = [m4[t, rows, :].astype(F32) for t in range(NY)]
        s = sum(jnp.sum(v, axis=1, keepdims=True) for v in parts) / D
        q = sum(jnp.sum(v * v, axis=1, keepdims=True) for v in parts) / D
        r = lax.rsqrt(q - s * s + norm_eps)
        for t in range(NY):
            nf[rows, t * CH : (t + 1) * CH] = (
                (parts[t] - s) * r * gbs[t, 0:1, :] + gbs[t, 1:2, :]
            ).astype(BF)
        return carry

    lax.fori_loop(0, ROWS // 32, norm_rows, 0)
    a_last()
    b_done()
    a_done()

    def up(j, carry):
        lanes = pl.ds(pl.multiple_of(DA + j * 256, 128), 256)
        f = dot(nf[...], w[:, :, :, :, lanes].reshape(D, 256))
        gv[8 : 8 + ROWS, pl.ds(pl.multiple_of(j * 256, 256), 256)] = f
        return carry

    lax.fori_loop(0, 2 * UNITS // 256, up, 0)
    tail = pl.ds(ROWS, 8)

    to_sib = copy_to(gv.at[tail], stat.at[0], sib, "t")
    to_next = pltpu.make_async_remote_copy(
        src_ref=gv.at[tail], dst_ref=stat.at[0], send_sem=ssem.at[len(sends) - 1],
        recv_sem=rsem.at[rid("t")], device_id=nexto, device_id_type=MESH,
    )

    @pl.when(c == 0)
    def _():
        to_sib.start()

    @pl.when(c == 1)
    def _():
        to_next.start()

    def conv_block(r0):
        here = dcol[8 + r0 : 8 + r0 + 128, :]
        one = (dcol[7 + r0 : 7 + r0 + 128, :] == here).astype(F32)
        two = (dcol[6 + r0 : 6 + r0 + 128, :] == here).astype(F32)

        def cols(j, carry):
            def mix(taps, base):
                lanes = pl.ds(pl.multiple_of(base + j * 128, 128), 128)
                a0 = gv[6 + r0 : 6 + r0 + 128, lanes]
                a1 = gv[7 + r0 : 7 + r0 + 128, lanes]
                a2 = gv[8 + r0 : 8 + r0 + 128, lanes]
                t = taps[:, pl.ds(pl.multiple_of(j * 128, 128), 128)].astype(F32)
                return t[0:1] * a0 * two + t[1:2] * a1 * one + t[2:3] * a2

            g = mix(cg_ref, 0)
            v = mix(cv_ref, UNITS)
            act = 0.5 * g * (1.0 + jnp.tanh(0.7978845608028654 * (g + 0.044715 * (g * g * g))))
            hid[r0 : r0 + 128, pl.ds(pl.multiple_of(j * 128, 128), 128)] = (v * act).astype(BF)
            return carry

        lax.fori_loop(0, UNITS // 128, cols, 0)

    for d in f_taps:
        d.wait()
    conv_block(256)
    conv_block(128)
    arrive(stat.at[0], "t")
    gv[0:8, :] = jnp.where(sp >= 1, stat[0], 0.0)
    conv_block(0)

    def unit_share(t):
        rows = pl.ds(2 * t, 2)
        da = w[rows, :, :, :, 0:DA].reshape(CH, DA)
        db = w[rows, :, :, :, LA + UNITS : LW].reshape(CH, UNITS - DA)
        return dot_nt(hid[:, 0:DA], da) + dot_nt(hid[:, DA:UNITS], db)

    settle(sends[mark : mark + 6])
    early = len(sends)

    def settle_early():
        settle(d for d in sends[:mark] if d is not None)
        settle(sends[mark + 6 : early])
        copy_at(docs.at[0], docs.at[1], sib, "d1", S_ALT + 1).wait_send()
        copy_at(docs.at[0], docs.at[3], sib, "d3", S_ALT + 2).wait_send()
        copy_at(packs.at[2], packs.at[3], sib, "s3", S_ALT + 3).wait_send()

        @pl.when(c == 0)
        def _():
            copy_at(packs.at[0], packs.at[1], sib, "l1", S_ALT).wait_send()
            for i, at in enumerate(zero_only):
                part = quarter(3, 0, 0, QR if i < 2 else QR // 2)
                copy_at(part, part, yp, "l3", at).wait_send()

        @pl.when(c == 1)
        def _():
            copy_at(quarter(2, 0), quarter(3, 0), nexto, "l3", S_ALT).wait_send()

    total_two = shared_sum(unit_share, "u", ra2, rb2, settle_early, lambda: None)
    mixed = (
        residual_scale * nf[:, pl.ds(pl.multiple_of(y * CH, CH), CH)].astype(F32) + total_two
    )
    own[...] = mixed
    s = jnp.sum(mixed, axis=1, keepdims=True)
    q = jnp.sum(mixed * mixed, axis=1, keepdims=True)
    both = jnp.where(lane == 0, s, jnp.where(lane == 1, q, 0.0))
    stats[y] = both.T[0:8, :]
    same(stats.at[y], yp, "qm")
    same(stats.at[y], ym, "qp")
    same(stats.at[y], yy, "q2")
    settle(sends[early:])
    arrive(stats.at[wrap(y - 1, NY)], "qm")
    arrive(stats.at[wrap(y + 1, NY)], "qp")
    arrive(stats.at[wrap(y + 2, NY)], "q2")
    tot = (stats[0] + stats[1]) + (stats[2] + stats[3])
    back = jnp.concatenate([tot, jnp.zeros((120, ROWS), F32)], axis=0).T
    s = back[:, 0:1] / D
    q = back[:, 1:2] / D
    r = lax.rsqrt(q - s * s + norm_eps)
    out_ref[...] = ((own[...] - s) * r * gb_ref[2:3, :] + gb_ref[3:4, :]).astype(BF)


def local(
    residual, query_nope, query_rope, latent, rope_key, doc_ids, key_up, value_up, out_proj,
    norm1_gain, norm1_bias, ffn_gate, ffn_value, conv_gate, conv_value, ffn_down,
    norm2_gain, norm2_bias,
):
    rows = latent.shape[0]
    turn = rope_base_freq ** (-np.arange(0, ROPE, 2, dtype=np.float64) / ROPE)
    turn = jnp.asarray(np.tile(np.tile(turn, 4)[None], (8, 1)).astype(np.float32))

    anyspec = pl.BlockSpec(memory_space=pl.ANY)
    vspec = pl.BlockSpec(memory_space=pltpu.VMEM)
    V = pltpu.VMEM
    return pl.pallas_call(
        layer_kernel,
        out_shape=jax.ShapeDtypeStruct((rows, CH), BF),
        in_specs=[anyspec] * 19,
        out_specs=vspec,
        scratch_shapes=[
            V((ROPE, ROWS), BF),
            V((CH,), BF),
            V((CH,), BF),
            V((CH,), BF),
            V((CH,), BF),
            V((ROWS,), jnp.int32),
            V((CONV, UNITS), BF),
            V((CONV, UNITS), BF),
            V((8, 128), F32),
            V((8, CH), F32),
            V((ROWS, 128), F32),
            V((ROWS, 128), F32),
            V((4, ROWS, PACKW), BF),
            V((ROWS, 1024), BF),
            V((ROWS, CH), BF),
            V((ROWS, 1024), BF),
            V((512, 1024), BF),
            V((512, 1024), BF),
            V((1024, D), BF),
            V((ROWS, CH), BF),
            V((NZ, NX, 2, 32, LW), BF),
            V((NY, 8, CH), F32),
            V((ROWS, 1024), BF),
            V((8, ROWS, 128), F32),
            V((8, ROWS, 128), F32),
            V((8, ROWS, 128), F32),
            V((8 + ROWS, 128), F32),
            V((4, 8, ROWS), F32),
            V((ROWS, ROWS), F32),
            V((ROWS, CH), BF),
            V((ROWS, CH), BF),
            V((ROWS, CH), BF),
            V((HALF, CH), F32),
            V((HALF, CH), F32),
            V((ROWS, CH), F32),
            V((2, HALF, CH), BF),
            V((2, ROWS, CH), BF),
            V((2, HALF, CH), BF),
            V((2, ROWS, CH), BF),
            V((NY, ROWS, CH), BF),
            V((ROWS, D), BF),
            V((8 + ROWS, 2 * UNITS), F32),
            V((ROWS, UNITS), BF),
            V((1, 8, 2 * UNITS), F32),
            V((NY, 8, ROWS), F32),
            pltpu.SemaphoreType.DMA((24,)),
            pltpu.SemaphoreType.DMA((N_SEND,)),
            pltpu.SemaphoreType.DMA((N_RECV,)),
        ],
        compiler_params=pltpu.CompilerParams(
            collective_id=0, has_side_effects=True, vmem_limit_bytes=54 * 1024 * 1024
        ),
    )(
        latent, query_nope, query_rope, key_up, value_up, out_proj, residual,
        ffn_gate, ffn_value, ffn_down.T, rope_key.T, norm1_gain, norm1_bias, norm2_gain, norm2_bias,
        doc_ids, conv_gate, conv_value, turn,
    )


def solution(mesh):
    placed = (
        P("sp", "tp"),
        P("sp", "tp"),
        P("sp", "tp"),
        P("sp", None),
        P("sp", None),
        P("sp"),
        P(None, "tp"),
        P(None, "tp"),
        P("tp", None),
        P("tp"),
        P("tp"),
        P("sp", "tp"),
        P("sp", "tp"),
        P(None, "tp"),
        P(None, "tp"),
        P("tp", "sp"),
        P("tp"),
        P("tp"),
    )
    return jax.shard_map(
        local, mesh=mesh, in_specs=placed, out_specs=P("sp", "tp"), check_vma=False
    )
```

```python
import jax
import jax.numpy as jnp
import numpy as np
from jax import lax
from jax.experimental import pallas as pl
from jax.experimental.pallas import tpu as pltpu
from jax.sharding import PartitionSpec as P

D = 2048
NOPE = 128
ROPE = 64
VDIM = 128
CONV = 3
REACH = 3

norm_eps = 1e-05
residual_scale = 8.0**0.25
rope_base_freq = 10000.0
masked_score = -1e30
SCALE2 = (NOPE + ROPE) ** (-0.5) * 1.4426950408889634

NX, NZ, NY = 4, 8, 4
ROWS = 384
HALF = ROWS // 2
LEAD = 16
CH = 512
UNITS = 1408
DA = 256
LA = DA + UNITS
LW = 3 * UNITS
PACKW = 640
GROUP = 8
N_SEND = 128
N_RECV = 128
S_ALT = N_SEND - 4
MESH = pl.DeviceIdType.MESH
BF = jnp.bfloat16
F32 = jnp.float32


def dot(a, b):
    return jnp.dot(a, b, preferred_element_type=F32)


def dot_nt(a, b):
    return lax.dot_general(a, b, (((1,), (1,)), ((), ())), preferred_element_type=F32)


def layer_kernel(
    lat_h, qn_h, qr_h, kup_h, vup_h, op_h, res_h, gate_h, value_h, down_h,
    key_h, g1_h, b1_h, g2_h, b2_h, doc_h, cg_h, cv_h, freq_h,
    out_ref,
    key_ref, v0, v1, v2, v3, doc_ref, cg_ref, cv_ref, freq_ref, gb_ref, cos_ref, sin_ref,
    packs, qn, qraw, qr, kup, vup, op, res, w, gbs, att, acc, mrun, lrun, dcol, docs, bias,
    sa, sp_buf, sm_buf, pfp, pfm, own, ra, rb, ra2, rb2, m4, nf, gv, hid, before_rows, stats,
    lsem, ssem, rsem,
):
    sp = lax.axis_index("sp")
    y = lax.axis_index("tp")
    c = lax.rem(sp, 2)
    k = lax.div(sp, 2)
    x = lax.rem(k, NX)
    z = lax.div(k, NX)

    def wrap(v, n):
        return lax.rem(v + n, n)

    def dev(zz, xx, cc, yy):
        return ((wrap(zz, NZ) * NX + wrap(xx, NX)) * 2 + cc, wrap(yy, NY))

    def chip(kk, cc):
        return (wrap(kk, NZ * NX) * 2 + cc, y)

    xp, xm = dev(z, x + 1, c, y), dev(z, x - 1, c, y)
    zp, zm = dev(z + 1, x, c, y), dev(z - 1, x, c, y)
    sib = dev(z, x, 1 - c, y)
    yp, ym, yy = dev(z, x, c, y + 1), dev(z, x, c, y - 1), dev(z, x, c, y + 2)
    nextc, prevc = chip(k + 1, c), chip(k - 1, c)
    nexto, prevo = chip(k + 1, 1 - c), chip(k - 1, 1 - c)

    local = []
    def fetch(src, dst):
        d = pltpu.make_async_copy(src, dst, lsem.at[len(local)])
        d.start()
        local.append(d)
        return d
    f_small = [
        fetch(key_h, key_ref),
        fetch(freq_h, freq_ref),
        fetch(doc_h, doc_ref),
        fetch(g1_h, v0),
        fetch(b1_h, v1),
        fetch(g2_h, v2),
        fetch(b2_h, v3),
    ]
    f_lat = fetch(lat_h, packs.at[0, :, pl.ds(0, 512)])
    mine = w.at[z, x, c]
    f_w = [
        fetch(gate_h, mine.at[:, pl.ds(DA, UNITS)]),
        fetch(value_h, mine.at[:, pl.ds(LA, UNITS)]),
        fetch(down_h.at[:, pl.ds(0, DA)], mine.at[:, pl.ds(0, DA)]),
        fetch(down_h.at[:, pl.ds(DA, UNITS - DA)], mine.at[:, pl.ds(LA + UNITS, UNITS - DA)]),
    ]
    f_qr = fetch(qr_h, qraw)
    f_kup = fetch(kup_h, kup)
    f_qn = fetch(qn_h, qn)
    f_vup = fetch(vup_h, vup)
    f_taps = [fetch(cg_h, cg_ref), fetch(cv_h, cv_ref)]
    f_op = fetch(op_h, op)
    f_res = fetch(res_h, res)

    barrier = pltpu.get_barrier_semaphore()
    peers = (
        xp, xm, zp, zm, sib, yp, ym, yy, nextc, prevc, nexto, prevo,
        chip(k + 2, 1 - c), chip(k - 2, 1 - c),
    )
    for p in peers:
        pl.semaphore_signal(barrier, inc=1, device_id=p, device_id_type=MESH)
    lane = lax.broadcasted_iota(jnp.int32, (ROWS, 128), 1)
    front = lax.rem(lane, ROPE) < ROPE // 2

    def turned(v):
        swapped = jnp.where(front, pltpu.roll(v, 128 - ROPE // 2, 1), pltpu.roll(v, ROPE // 2, 1))
        return v * cos_ref[...] + swapped * sin_ref[...]

    for d in f_small:
        d.wait()
    place = lax.broadcasted_iota(jnp.int32, (ROWS, 128), 0) + sp * ROWS
    angle = place.astype(F32) * freq_ref[0:1, :]
    cos_ref[...] = jnp.cos(angle)
    sin_ref[...] = jnp.where(front, -1.0, 1.0) * jnp.sin(angle)
    key = key_ref[...].astype(F32)
    packs[0, :, 512:640] = (turned(jnp.concatenate([key, key], axis=0).T) * SCALE2).astype(BF)
    docs[0] = jnp.broadcast_to(doc_ref[...].astype(F32).reshape(1, ROWS), (8, ROWS))
    gb_ref[...] = jnp.concatenate(
        [v[...].astype(F32).reshape(1, CH) for v in (v0, v1, v2, v3)] + [jnp.zeros((4, CH), F32)], axis=0
    )
    def doc_column(slot):
        return jnp.concatenate([docs[slot], jnp.zeros((120, ROWS), F32)], axis=0).T[:, 0:1]

    pl.semaphore_wait(barrier, len(peers))

    sends = []
    zero_only = []
    names = {}

    def rid(name):
        return names.setdefault(name, len(names))

    def copy_to(src, dst, to, name):
        d = pltpu.make_async_remote_copy(
            src_ref=src, dst_ref=dst, send_sem=ssem.at[len(sends)],
            recv_sem=rsem.at[rid(name)], device_id=to, device_id_type=MESH,
        )
        sends.append(d)
        return d

    def copy_at(src, dst, to, name, at):
        return pltpu.make_async_remote_copy(
            src_ref=src, dst_ref=dst, send_sem=ssem.at[at],
            recv_sem=rsem.at[rid(name)], device_id=to, device_id_type=MESH,
        )

    def send(src, dst, to, name):
        copy_to(src, dst, to, name).start()

    def arrive(dst, name):
        pltpu.make_async_remote_copy(
            src_ref=dst, dst_ref=dst, send_sem=ssem.at[0],
            recv_sem=rsem.at[rid(name)], device_id=sib, device_id_type=MESH,
        ).wait_recv()

    def wa(dz, dx):
        return w.at[wrap(z + dz, NZ), wrap(x + dx, NX), c, :, pl.ds(0, LA)]

    def za(dz, cc, lo=0, n=NX):
        return w.at[wrap(z + dz, NZ), pl.ds(lo, n), cc, :, pl.ds(0, LA)]

    def wb(dz, lo=LA, n=LW - LA):
        return w.at[wrap(z + dz, NZ), x, c, :, pl.ds(lo, n)]

    def xb(dx, cc, lo=0, n=NZ):
        return w.at[pl.ds(lo, n), wrap(x + dx, NX), cc, :, pl.ds(LA, LW - LA)]

    BH = (LW - LA) // 2
    HX = NX // 2

    def bp(dz, dx):
        return w.at[wrap(z + dz, NZ), wrap(x + dx, NX), c, :, pl.ds(LA, LW - LA)]

    def same(ref, to, name):
        send(ref, ref, to, name)

    def a_start():
        same(wa(0, 0), xp, "a1m")
        same(wa(0, 0), xm, "a1p")

    def za_piece(dx):
        same(wa(0, dx), zp, f"z1m{dx}")
        same(wa(0, dx), zm, f"z1p{dx}")

    def a_one():
        arrive(wa(0, 1), "a1p")
        same(wa(0, 1), xm, "a2p")
        za_piece(1)

    def a_two():
        arrive(wa(0, -1), "a1m")
        za_piece(-1)
        arrive(wa(0, 2), "a2p")
        za_piece(2)
        same(za(0, c), sib, "sz0")

    def a_step(s):
        if s == 1:
            for dx in (0, 1, -1, 2):
                arrive(wa(-1, dx), f"z1m{dx}")
                arrive(wa(1, dx), f"z1p{dx}")
        else:
            arrive(za(-s, c), f"z{s}m")
            arrive(za(s, c), f"z{s}p")
        if s < 3:
            same(za(-s, c), zp, f"z{s + 1}m")
            same(za(s, c), zm, f"z{s + 1}p")
        else:
            same(za(-s, c, 0, HX), zp, "z4m")
            same(za(s, c, HX, HX), zm, "z4p")
        same(za(-s, c), sib, f"sz{s}m")
        same(za(s, c), sib, f"sz{s}p")

    def a_last():
        arrive(za(4, c, 0, HX), "z4m")
        arrive(za(4, c, HX, HX), "z4p")
        same(za(4, c), sib, "sz4")

    def a_done():
        arrive(za(0, 1 - c), "sz0")
        for s in (1, 2, 3):
            arrive(za(-s, 1 - c), f"sz{s}m")
            arrive(za(s, 1 - c), f"sz{s}p")
        arrive(za(4, 1 - c), "sz4")

    def bx_piece(dz):
        same(bp(dz, 0), xp, f"x1m{dz}")
        same(bp(dz, 0), xm, f"x1p{dz}")

    def b_start():
        same(wb(0), zp, "b1m")
        same(wb(0), zm, "b1p")

    def b_step(s):
        arrive(wb(-s), f"b{s}m")
        arrive(wb(s), f"b{s}p")
        if s < 3:
            same(wb(-s), zp, f"b{s + 1}m")
            same(wb(s), zm, f"b{s + 1}p")
        else:
            same(wb(-s, LA, BH), zp, "b4m")
            same(wb(s, LA + BH, BH), zm, "b4p")
        bx_piece(-s)
        bx_piece(s)

    def b_turn():
        arrive(wb(4, LA, BH), "b4m")
        arrive(wb(4, LA + BH, BH), "b4p")
        bx_piece(4)
        same(xb(0, c), sib, "sx0")

    DOWN = (-1, -2, -3, 4)

    def b_cross(i):
        up, down = i, DOWN[i]
        arrive(bp(up, -1), f"x1m{up}")
        same(bp(up, -1), xp, f"x2m{up}")
        arrive(bp(down, 1), f"x1p{down}")
        same(bp(down, 1), xm, f"x2p{down}")
        same(bp(up, -1), sib, "sx1m")
        same(bp(down, 1), sib, "sx1p")

    def b_collect(i):
        up, down = i, DOWN[i]
        arrive(bp(down, -1), f"x1m{down}")
        arrive(bp(up, 1), f"x1p{up}")
        same(bp(down, -1), sib, "sx1m")
        same(bp(up, 1), sib, "sx1p")

    def b_last(i):
        up, down = i, DOWN[i]
        arrive(bp(up, 2), f"x2m{up}")
        arrive(bp(down, 2), f"x2p{down}")
        same(bp(up, 2), sib, "sx2")
        same(bp(down, 2), sib, "sx2")

    def b_done():
        arrive(xb(0, 1 - c), "sx0")
        arrive(xb(-1, 1 - c), "sx1m")
        arrive(xb(1, 1 - c), "sx1p")
        arrive(xb(2, 1 - c), "sx2")

    QR = ROWS // NY

    def quarter(slot, dy, lo=0, n=QR):
        return packs.at[slot, pl.ds(pl.multiple_of(wrap(y + dy, NY) * QR + lo, 16), n)]

    def spread(slot, tag):
        def one():
            arrive(quarter(slot, 0), tag)
            same(quarter(slot, 0), yp, tag + "1m")
            same(quarter(slot, 0), ym, tag + "1p")

        def two():
            arrive(quarter(slot, -1), tag + "1m")
            same(quarter(slot, -1, 0, QR // 2), yp, tag + "2m")
            arrive(quarter(slot, 1), tag + "1p")
            same(quarter(slot, 1, QR // 2, QR // 2), ym, tag + "2p")

        def three():
            arrive(quarter(slot, 2, 0, QR // 2), tag + "2m")
            arrive(quarter(slot, 2, QR // 2, QR // 2), tag + "2p")

        return one, two, three

    f_lat.wait()
    send(quarter(0, 0), quarter(2, 0), nextc, "l2")
    send(docs.at[0], docs.at[2], nextc, "d2")
    for d in f_w:
        d.wait()
    a_start()
    b_start()
    bx_piece(0)
    za_piece(0)

    @pl.when(c == 0)
    def _():
        copy_at(packs.at[0], packs.at[1], sib, "l1", S_ALT).start()
        copy_at(docs.at[0], docs.at[1], sib, "d1", S_ALT + 1).start()
        copy_at(docs.at[0], docs.at[3], nexto, "d3", S_ALT + 2).start()

    @pl.when(c == 1)
    def _():
        copy_at(docs.at[0], docs.at[1], nexto, "d1", S_ALT + 1).start()
        copy_at(docs.at[0], docs.at[3], chip(k + 2, 0), "d3", S_ALT + 2).start()

    send(gb_ref, gbs.at[y], yp, "gm")
    send(gb_ref, gbs.at[y], ym, "gp")
    send(gb_ref, gbs.at[y], yy, "g2")
    dcol[8 : 8 + ROWS, :] = jnp.broadcast_to(doc_column(0), (ROWS, 128))
    f_qr.wait()
    for t in range(4):
        v = turned(qraw[:, t * 128 : t * 128 + 128].astype(F32))
        qr[:, t * 256 : t * 256 + 128] = jnp.where(lane < ROPE, v, 0.0).astype(BF)
        qr[:, t * 256 + 128 : t * 256 + 256] = jnp.where(lane >= ROPE, v, 0.0).astype(BF)

    def attend(slot, back, kind, first=False, last=False):
        kdoc = jnp.where(sp >= back, docs[slot, 0:1, :], -1.0)
        ok = dcol[8 : 8 + ROWS, 0:1] == kdoc
        if kind == "diag":
            qi_pos = lax.broadcasted_iota(jnp.int32, (ROWS, ROWS), 0)
            ki_pos = lax.broadcasted_iota(jnp.int32, (ROWS, ROWS), 1)
            ok = ok & (ki_pos <= qi_pos)
        bias[...] = jnp.where(ok, 0.0, masked_score)
        ones = jnp.ones((ROWS, 128), BF)

        def body(group, carry):
            lat = packs[slot, :, 0:512]
            kr = packs[slot, :, 512:640]
            lanes, states, results = [], [], []
            for hh in range(GROUP):
                h = group * GROUP + hh
                lanes.append(pl.ds(pl.multiple_of(h * 128, 128), 128))
                if not first:
                    states.append((mrun[h], lrun[h], acc[h]))
            pairs = {}

            def keys(i):
                both = pl.ds(pl.multiple_of((group * GROUP + 2 * i) * 128, 256), 256)
                pairs[i] = (
                    (dot(lat, kup[:, both]) * SCALE2).astype(BF),
                    dot(lat, vup[:, both]).astype(BF),
                )

            def score(hh):
                k2 = pairs[hh // 2][0][:, hh % 2 * 128 : hh % 2 * 128 + 128]
                q = jnp.concatenate([qn[:, lanes[hh]], qr[:, lanes[hh]]], axis=1)
                return dot_nt(q, jnp.concatenate([k2, kr], axis=1)) + bias[...]

            keys(0)
            ahead = score(0)
            for hh in range(GROUP):
                s = ahead
                if hh % 2 == 0 and hh + 2 < GROUP:
                    keys(hh // 2 + 1)
                if hh + 1 < GROUP:
                    ahead = score(hh + 1)
                v2 = pairs[hh // 2][1][:, hh % 2 * 128 : hh % 2 * 128 + 128]
                mx = jnp.max(s, axis=1, keepdims=True)
                if first:
                    mnew = jnp.broadcast_to(mx, (ROWS, 128))
                else:
                    mnew = jnp.maximum(states[hh][0], mx)
                p = jnp.exp2(s - mnew[:, 0:1])
                o = dot(p.astype(BF), jnp.concatenate([v2, ones], axis=1))
                o, total = o[:, 0:128], o[:, 128:256]
                if not first:
                    alpha = jnp.exp2(states[hh][0] - mnew)
                    total = states[hh][1] * alpha + total
                    o = states[hh][2] * alpha + o
                results.append((mnew, total, o))
            for hh in range(GROUP):
                h = group * GROUP + hh
                mnew, total, o = results[hh]
                if last:
                    att[:, lanes[hh]] = (o / total).astype(BF)
                else:
                    mrun[h] = mnew
                    lrun[h] = total
                    acc[h] = o
            return carry

        lax.fori_loop(0, 8 // GROUP, body, 0)

    f_kup.wait()
    f_qn.wait()
    f_vup.wait()
    slot_two = spread(2, "l2")
    slot_three = spread(3, "l3")
    attend(0, 0, "diag", first=True)
    slot_two[0]()

    @pl.when(c == 1)
    def _():
        copy_at(quarter(2, 0), quarter(3, 0), nexto, "l3", S_ALT).start()

    a_one()
    b_step(1)
    slot_two[1]()
    a_two()
    slot_two[2]()

    @pl.when(c == 0)
    def _():
        copy_at(packs.at[2], packs.at[3], sib, "s3", S_ALT + 3).start()
        before = len(sends)
        slot_three[0]()
        for i in range(before, len(sends)):
            zero_only.append(i)
            sends[i] = None

    @pl.when(c == 1)
    def _():
        copy_at(packs.at[2], packs.at[1], sib, "l1", S_ALT + 3).start()

    arrive(docs.at[2], "d2")
    attend(2, 2, "full")
    b_step(2)
    b_cross(0)

    @pl.when(c == 0)
    def _():
        before = len(sends)
        slot_three[1]()
        for i in range(before, len(sends)):
            zero_only.append(i)
            sends[i] = None

    arrive(packs.at[1], "l1")
    arrive(docs.at[1], "d1")
    before = jnp.where(sp >= 1, doc_column(1)[ROWS - 8 : ROWS, :], -1.0)
    dcol[0:8, :] = jnp.broadcast_to(before, (8, 128))
    attend(1, 1, "full")
    b_step(3)
    a_step(1)
    arrive(docs.at[3], "d3")

    @pl.when(c == 0)
    def _():
        slot_three[2]()

    @pl.when(c == 1)
    def _():
        arrive(packs.at[3], "s3")

    attend(3, 3, "far", last=True)

    UP, LOW = pl.ds(0, HALF), pl.ds(HALF, HALF)

    def far_all(chunk, tag, ra):
        sa[...] = chunk(wrap(y + 2, NY), pl.ds(0, ROWS)).astype(BF)
        send(sa.at[UP], ra.at[0], yp, tag + "am")
        send(sa.at[LOW], ra.at[1], ym, tag + "ap")

    def near_all(chunk, tag, rb):
        f = chunk(wrap(y + 1, NY), pl.ds(0, ROWS))
        pfp[...] = f[:HALF]
        sp_buf[LOW, :] = f[HALF:].astype(BF)
        send(sp_buf.at[LOW], rb.at[0, LOW], yp, tag + "bm1")
        f = chunk(wrap(y - 1, NY), pl.ds(0, ROWS))
        pfm[...] = f[HALF:]
        sm_buf[UP, :] = f[:HALF].astype(BF)
        send(sm_buf.at[UP], rb.at[1, UP], ym, tag + "bp0")

    def forward(tag, ra, rb):
        arrive(ra.at[0], tag + "am")
        sp_buf[UP, :] = (pfp[...] + ra[0].astype(F32)).astype(BF)
        send(sp_buf.at[UP], rb.at[0, UP], yp, tag + "bm0")
        arrive(ra.at[1], tag + "ap")
        sm_buf[LOW, :] = (pfm[...] + ra[1].astype(F32)).astype(BF)
        send(sm_buf.at[LOW], rb.at[1, LOW], ym, tag + "bp1")

    def collected(tag, rb):
        arrive(rb.at[0, LOW], tag + "bm1")
        arrive(rb.at[1, UP], tag + "bp0")
        arrive(rb.at[0, UP], tag + "bm0")
        arrive(rb.at[1, LOW], tag + "bp1")
        return own[...] + rb[0].astype(F32) + rb[1].astype(F32)

    def settle(ds):
        for d in ds:
            d.wait_send()

    f_op.wait()
    f_res.wait()

    def head_share(t, rows):
        return dot(att[rows, :], op[:, pl.ds(pl.multiple_of(t * CH, CH), CH)])

    mark = len(sends)

    far_all(head_share, "p", ra)
    near_all(head_share, "p", rb)
    own[...] = head_share(y, pl.ds(0, ROWS))
    b_turn()
    forward("p", ra, rb)
    b_cross(1)
    b_cross(2)
    a_step(2)
    total_one = collected("p", rb)
    m4[y] = (residual_scale * res[...].astype(F32) + total_one).astype(BF)

    def piece(dy, lo):
        return m4.at[wrap(y + dy, NY), pl.ds(lo, HALF)]

    same(piece(0, 0), yp, "m1m0")
    same(piece(0, HALF), ym, "m1p1")
    same(piece(0, HALF), yp, "m1m1")
    same(piece(0, 0), ym, "m1p0")
    b_cross(3)
    arrive(piece(-1, 0), "m1m0")
    same(piece(-1, 0), yp, "m2m")
    arrive(piece(1, HALF), "m1p1")
    same(piece(1, HALF), ym, "m2p")
    arrive(gbs.at[wrap(y - 1, NY)], "gm")
    arrive(gbs.at[wrap(y + 1, NY)], "gp")
    arrive(gbs.at[wrap(y + 2, NY)], "g2")
    gbs[y] = gb_ref[...]
    a_step(3)
    for i in range(4):
        b_collect(i)
    arrive(piece(-1, HALF), "m1m1")
    arrive(piece(1, 0), "m1p0")
    for i in range(4):
        b_last(i)
    arrive(piece(2, 0), "m2m")
    arrive(piece(2, HALF), "m2p")

    def norm_of(src, rows, out_rows):
        parts = [src[t, rows, :].astype(F32) for t in range(NY)]
        s = sum(jnp.sum(v, axis=1, keepdims=True) for v in parts) / D
        q = sum(jnp.sum(v * v, axis=1, keepdims=True) for v in parts) / D
        r = lax.rsqrt(q - s * s + norm_eps)
        for t in range(NY):
            nf[out_rows, t * CH : (t + 1) * CH] = (
                (parts[t] - s) * r * gbs[t, 0:1, :] + gbs[t, 1:2, :]
            ).astype(BF)

    def norm_rows(i, carry):
        first = pl.multiple_of(i * 32, 32)
        norm_of(m4, pl.ds(first, 32), pl.ds(pl.multiple_of(first + LEAD, 16), 32))
        return carry

    tail = m4.at[:, pl.ds(ROWS - LEAD, LEAD), :]
    copy_to(tail, before_rows, sib, "t")
    tail_at = len(sends) - 1

    @pl.when(c == 0)
    def _():
        copy_at(tail, before_rows, sib, "t", tail_at).start()

    @pl.when(c == 1)
    def _():
        copy_at(tail, before_rows, nexto, "t", tail_at).start()

    a_last()
    lax.fori_loop(0, ROWS // 32, norm_rows, 0)
    b_done()
    a_done()

    arrive(before_rows, "t")
    norm_of(before_rows, pl.ds(0, LEAD), pl.ds(0, LEAD))
    for d in f_taps:
        d.wait()

    def block(base, j):
        return pl.ds(pl.multiple_of(base + j * 128, 128), 128)

    def up(j):
        both = jnp.concatenate([w[:, :, :, :, block(DA, j)], w[:, :, :, :, block(LA, j)]], axis=4)
        f = dot(nf[...], both.reshape(D, 256))
        gv[:, block(0, j)] = f[:, 0:128]
        gv[:, block(UNITS, j)] = f[:, 128:256]

    def conv(j):
        here = dcol[8 : 8 + ROWS, :]
        near = (dcol[7 : 7 + ROWS, :] == here).astype(F32)
        far = (dcol[6 : 6 + ROWS, :] == here).astype(F32)

        def mix(taps, base):
            a0 = gv[LEAD - 2 : LEAD - 2 + ROWS, block(base, j)]
            a1 = gv[LEAD - 1 : LEAD - 1 + ROWS, block(base, j)]
            a2 = gv[LEAD : LEAD + ROWS, block(base, j)]
            t = taps[:, block(0, j)].astype(F32)
            return t[0:1] * a0 * far + t[1:2] * a1 * near + t[2:3] * a2

        g = mix(cg_ref, 0)
        v = mix(cv_ref, UNITS)
        act = 0.5 * g * (1.0 + jnp.tanh(0.7978845608028654 * (g + 0.044715 * (g * g * g))))
        hid[:, block(0, j)] = (v * act).astype(BF)

    def step(j, carry):
        conv(j - 1)
        up(j)
        return carry

    up(0)
    lax.fori_loop(1, UNITS // 128, step, 0)
    conv(UNITS // 128 - 1)

    def unit_share(t, rows):
        part = pl.ds(2 * t, 2)
        da = w[part, :, :, :, 0:DA].reshape(CH, DA)
        db = w[part, :, :, :, LA + UNITS : LW].reshape(CH, UNITS - DA)
        return dot_nt(hid[rows, 0:DA], da) + dot_nt(hid[rows, DA:UNITS], db)

    settle(sends[mark : mark + 6])
    early = len(sends)

    def settle_early():
        settle(d for d in sends[:mark] if d is not None)
        settle(sends[mark + 6 : early])
        copy_at(docs.at[0], docs.at[1], sib, "d1", S_ALT + 1).wait_send()
        copy_at(docs.at[0], docs.at[3], sib, "d3", S_ALT + 2).wait_send()
        copy_at(packs.at[2], packs.at[3], sib, "s3", S_ALT + 3).wait_send()

        @pl.when(c == 0)
        def _():
            copy_at(packs.at[0], packs.at[1], sib, "l1", S_ALT).wait_send()
            for i, at in enumerate(zero_only):
                part = quarter(3, 0, 0, QR if i < 2 else QR // 2)
                copy_at(part, part, yp, "l3", at).wait_send()

        @pl.when(c == 1)
        def _():
            copy_at(quarter(2, 0), quarter(3, 0), nexto, "l3", S_ALT).wait_send()

    far_all(unit_share, "u", ra2)
    near_all(unit_share, "u", rb2)
    own[...] = unit_share(y, pl.ds(0, ROWS))
    settle_early()
    forward("u", ra2, rb2)
    total_two = collected("u", rb2)
    mixed = (
        residual_scale * nf[LEAD : LEAD + ROWS, pl.ds(pl.multiple_of(y * CH, CH), CH)].astype(F32) + total_two
    )
    own[...] = mixed
    s = jnp.sum(mixed, axis=1, keepdims=True)
    q = jnp.sum(mixed * mixed, axis=1, keepdims=True)
    both = jnp.where(lane == 0, s, jnp.where(lane == 1, q, 0.0))
    stats[y] = both.T[0:8, :]
    same(stats.at[y], yp, "qm")
    same(stats.at[y], ym, "qp")
    same(stats.at[y], yy, "q2")
    settle(sends[early:])
    arrive(stats.at[wrap(y - 1, NY)], "qm")
    arrive(stats.at[wrap(y + 1, NY)], "qp")
    arrive(stats.at[wrap(y + 2, NY)], "q2")
    tot = (stats[0] + stats[1]) + (stats[2] + stats[3])
    back = jnp.concatenate([tot, jnp.zeros((120, ROWS), F32)], axis=0).T
    s = back[:, 0:1] / D
    q = back[:, 1:2] / D
    r = lax.rsqrt(q - s * s + norm_eps)
    out_ref[...] = ((own[...] - s) * r * gb_ref[2:3, :] + gb_ref[3:4, :]).astype(BF)


def local(
    residual, query_nope, query_rope, latent, rope_key, doc_ids, key_up, value_up, out_proj,
    norm1_gain, norm1_bias, ffn_gate, ffn_value, conv_gate, conv_value, ffn_down,
    norm2_gain, norm2_bias,
):
    rows = latent.shape[0]
    turn = rope_base_freq ** (-np.arange(0, ROPE, 2, dtype=np.float64) / ROPE)
    turn = jnp.asarray(np.tile(np.tile(turn, 4)[None], (8, 1)).astype(np.float32))

    anyspec = pl.BlockSpec(memory_space=pl.ANY)
    vspec = pl.BlockSpec(memory_space=pltpu.VMEM)
    V = pltpu.VMEM
    return pl.pallas_call(
        layer_kernel,
        out_shape=jax.ShapeDtypeStruct((rows, CH), BF),
        in_specs=[anyspec] * 19,
        out_specs=vspec,
        scratch_shapes=[
            V((ROPE, ROWS), BF),
            V((CH,), BF),
            V((CH,), BF),
            V((CH,), BF),
            V((CH,), BF),
            V((ROWS,), jnp.int32),
            V((CONV, UNITS), BF),
            V((CONV, UNITS), BF),
            V((8, 128), F32),
            V((8, CH), F32),
            V((ROWS, 128), F32),
            V((ROWS, 128), F32),
            V((4, ROWS, PACKW), BF),
            V((ROWS, 1024), BF),
            V((ROWS, CH), BF),
            V((ROWS, 1024), BF),
            V((512, 1024), BF),
            V((512, 1024), BF),
            V((1024, D), BF),
            V((ROWS, CH), BF),
            V((NZ, NX, 2, 32, LW), BF),
            V((NY, 8, CH), F32),
            V((ROWS, 1024), BF),
            V((8, ROWS, 128), F32),
            V((8, ROWS, 128), F32),
            V((8, ROWS, 128), F32),
            V((8 + ROWS, 128), F32),
            V((4, 8, ROWS), F32),
            V((ROWS, ROWS), F32),
            V((ROWS, CH), BF),
            V((ROWS, CH), BF),
            V((ROWS, CH), BF),
            V((HALF, CH), F32),
            V((HALF, CH), F32),
            V((ROWS, CH), F32),
            V((2, HALF, CH), BF),
            V((2, ROWS, CH), BF),
            V((2, HALF, CH), BF),
            V((2, ROWS, CH), BF),
            V((NY, ROWS, CH), BF),
            V((LEAD + ROWS, D), BF),
            V((LEAD + ROWS, 2 * UNITS), F32),
            V((ROWS, UNITS), BF),
            V((NY, LEAD, CH), BF),
            V((NY, 8, ROWS), F32),
            pltpu.SemaphoreType.DMA((24,)),
            pltpu.SemaphoreType.DMA((N_SEND,)),
            pltpu.SemaphoreType.DMA((N_RECV,)),
        ],
        compiler_params=pltpu.CompilerParams(
            collective_id=0, has_side_effects=True, vmem_limit_bytes=54 * 1024 * 1024
        ),
    )(
        latent, query_nope, query_rope, key_up, value_up, out_proj, residual,
        ffn_gate, ffn_value, ffn_down.T, rope_key.T, norm1_gain, norm1_bias, norm2_gain, norm2_bias,
        doc_ids, conv_gate, conv_value, turn,
    )


def solution(mesh):
    placed = (
        P("sp", "tp"),
        P("sp", "tp"),
        P("sp", "tp"),
        P("sp", None),
        P("sp", None),
        P("sp"),
        P(None, "tp"),
        P(None, "tp"),
        P("tp", None),
        P("tp"),
        P("tp"),
        P("sp", "tp"),
        P("sp", "tp"),
        P(None, "tp"),
        P(None, "tp"),
        P("tp", "sp"),
        P("tp"),
        P("tp"),
    )
    return jax.shard_map(
        local, mesh=mesh, in_specs=placed, out_specs=P("sp", "tp"), check_vma=False
    )
```

```python
import jax
import jax.numpy as jnp
import numpy as np
from jax import lax
from jax.experimental import pallas as pl
from jax.experimental.pallas import tpu as pltpu
from jax.sharding import PartitionSpec as P

D = 2048
NOPE = 128
ROPE = 64
VDIM = 128
CONV = 3
REACH = 3

norm_eps = 1e-05
residual_scale = 8.0**0.25
rope_base_freq = 10000.0
masked_score = -1e30
SCALE2 = (NOPE + ROPE) ** (-0.5) * 1.4426950408889634

NX, NZ, NY = 4, 8, 4
ROWS = 384
HALF = ROWS // 2
LEAD = 16
PARTS = 4
CH = 512
UNITS = 1408
DA = 256
LA = DA + UNITS
LW = 3 * UNITS
PACKW = 640
GROUP = 8
N_SEND = 128
N_RECV = 128
S_ALT = N_SEND - 4
MESH = pl.DeviceIdType.MESH
BF = jnp.bfloat16
F32 = jnp.float32


def dot(a, b):
    return jnp.dot(a, b, preferred_element_type=F32)


def dot_nt(a, b):
    return lax.dot_general(a, b, (((1,), (1,)), ((), ())), preferred_element_type=F32)


def layer_kernel(
    lat_h, qn_h, qr_h, kup_h, vup_h, op_h, res_h, gate_h, value_h, down_h,
    key_h, g1_h, b1_h, g2_h, b2_h, doc_h, cg_h, cv_h, freq_h,
    out_ref,
    key_ref, v0, v1, v2, v3, doc_ref, cg_ref, cv_ref, freq_ref, gb_ref, cos_ref, sin_ref,
    packs, qn, qraw, qr, kup, vup, op, res, w, gbs, att, acc, mrun, lrun, dcol, docs, bias,
    sa, sp_buf, sm_buf, pfp, pfm, own, ra, rb, ra2, rb2, m4, nf, gv, hid, before_rows, stats,
    lsem, ssem, rsem,
):
    sp = lax.axis_index("sp")
    y = lax.axis_index("tp")
    c = lax.rem(sp, 2)
    k = lax.div(sp, 2)
    x = lax.rem(k, NX)
    z = lax.div(k, NX)

    def wrap(v, n):
        return lax.rem(v + n, n)

    def dev(zz, xx, cc, yy):
        return ((wrap(zz, NZ) * NX + wrap(xx, NX)) * 2 + cc, wrap(yy, NY))

    def chip(kk, cc):
        return (wrap(kk, NZ * NX) * 2 + cc, y)

    xp, xm = dev(z, x + 1, c, y), dev(z, x - 1, c, y)
    zp, zm = dev(z + 1, x, c, y), dev(z - 1, x, c, y)
    sib = dev(z, x, 1 - c, y)
    yp, ym, yy = dev(z, x, c, y + 1), dev(z, x, c, y - 1), dev(z, x, c, y + 2)
    nextc, prevc = chip(k + 1, c), chip(k - 1, c)
    nexto, prevo = chip(k + 1, 1 - c), chip(k - 1, 1 - c)

    local = []
    def fetch(src, dst):
        d = pltpu.make_async_copy(src, dst, lsem.at[len(local)])
        d.start()
        local.append(d)
        return d
    f_small = [
        fetch(key_h, key_ref),
        fetch(freq_h, freq_ref),
        fetch(doc_h, doc_ref),
        fetch(g1_h, v0),
        fetch(b1_h, v1),
        fetch(g2_h, v2),
        fetch(b2_h, v3),
    ]
    f_lat = fetch(lat_h, packs.at[0, :, pl.ds(0, 512)])
    mine = w.at[z, x, c]
    f_w = [
        fetch(gate_h, mine.at[:, pl.ds(DA, UNITS)]),
        fetch(value_h, mine.at[:, pl.ds(LA, UNITS)]),
        fetch(down_h.at[:, pl.ds(0, DA)], mine.at[:, pl.ds(0, DA)]),
        fetch(down_h.at[:, pl.ds(DA, UNITS - DA)], mine.at[:, pl.ds(LA + UNITS, UNITS - DA)]),
    ]
    f_qr = fetch(qr_h, qraw)
    f_kup = fetch(kup_h, kup)
    f_qn = fetch(qn_h, qn)
    f_vup = fetch(vup_h, vup)
    f_taps = [fetch(cg_h, cg_ref), fetch(cv_h, cv_ref)]
    f_op = fetch(op_h, op)
    f_res = fetch(res_h, res)

    barrier = pltpu.get_barrier_semaphore()
    peers = (
        xp, xm, zp, zm, sib, yp, ym, yy, nextc, prevc, nexto, prevo,
        chip(k + 2, 1 - c), chip(k - 2, 1 - c),
    )
    for p in peers:
        pl.semaphore_signal(barrier, inc=1, device_id=p, device_id_type=MESH)
    lane = lax.broadcasted_iota(jnp.int32, (ROWS, 128), 1)
    front = lax.rem(lane, ROPE) < ROPE // 2

    def turned(v):
        swapped = jnp.where(front, pltpu.roll(v, 128 - ROPE // 2, 1), pltpu.roll(v, ROPE // 2, 1))
        return v * cos_ref[...] + swapped * sin_ref[...]

    for d in f_small:
        d.wait()
    place = lax.broadcasted_iota(jnp.int32, (ROWS, 128), 0) + sp * ROWS
    angle = place.astype(F32) * freq_ref[0:1, :]
    cos_ref[...] = jnp.cos(angle)
    sin_ref[...] = jnp.where(front, -1.0, 1.0) * jnp.sin(angle)
    key = key_ref[...].astype(F32)
    packs[0, :, 512:640] = (turned(jnp.concatenate([key, key], axis=0).T) * SCALE2).astype(BF)
    docs[0] = jnp.broadcast_to(doc_ref[...].astype(F32).reshape(1, ROWS), (8, ROWS))
    gb_ref[...] = jnp.concatenate(
        [v[...].astype(F32).reshape(1, CH) for v in (v0, v1, v2, v3)] + [jnp.zeros((4, CH), F32)], axis=0
    )
    def doc_column(slot):
        return jnp.concatenate([docs[slot], jnp.zeros((120, ROWS), F32)], axis=0).T[:, 0:1]

    pl.semaphore_wait(barrier, len(peers))

    sends = []
    zero_only = []
    names = {}

    def rid(name):
        return names.setdefault(name, len(names))

    def copy_to(src, dst, to, name):
        d = pltpu.make_async_remote_copy(
            src_ref=src, dst_ref=dst, send_sem=ssem.at[len(sends)],
            recv_sem=rsem.at[rid(name)], device_id=to, device_id_type=MESH,
        )
        sends.append(d)
        return d

    def copy_at(src, dst, to, name, at):
        return pltpu.make_async_remote_copy(
            src_ref=src, dst_ref=dst, send_sem=ssem.at[at],
            recv_sem=rsem.at[rid(name)], device_id=to, device_id_type=MESH,
        )

    def send(src, dst, to, name):
        copy_to(src, dst, to, name).start()

    def arrive(dst, name):
        pltpu.make_async_remote_copy(
            src_ref=dst, dst_ref=dst, send_sem=ssem.at[0],
            recv_sem=rsem.at[rid(name)], device_id=sib, device_id_type=MESH,
        ).wait_recv()

    def wa(dz, dx):
        return w.at[wrap(z + dz, NZ), wrap(x + dx, NX), c, :, pl.ds(0, LA)]

    def za(dz, cc, lo=0, n=NX):
        return w.at[wrap(z + dz, NZ), pl.ds(lo, n), cc, :, pl.ds(0, LA)]

    def wb(dz, lo=LA, n=LW - LA):
        return w.at[wrap(z + dz, NZ), x, c, :, pl.ds(lo, n)]

    def xb(dx, cc, lo=0, n=NZ):
        return w.at[pl.ds(lo, n), wrap(x + dx, NX), cc, :, pl.ds(LA, LW - LA)]

    BH = (LW - LA) // 2
    HX = NX // 2

    def bp(dz, dx):
        return w.at[wrap(z + dz, NZ), wrap(x + dx, NX), c, :, pl.ds(LA, LW - LA)]

    def same(ref, to, name):
        send(ref, ref, to, name)

    def a_start():
        same(wa(0, 0), xp, "a1m")
        same(wa(0, 0), xm, "a1p")

    def za_piece(dx):
        same(wa(0, dx), zp, f"z1m{dx}")
        same(wa(0, dx), zm, f"z1p{dx}")

    def a_one():
        arrive(wa(0, 1), "a1p")
        same(wa(0, 1), xm, "a2p")
        za_piece(1)

    def a_two():
        arrive(wa(0, -1), "a1m")
        za_piece(-1)
        arrive(wa(0, 2), "a2p")
        za_piece(2)
        same(za(0, c), sib, "sz0")

    def a_step(s):
        if s == 1:
            for dx in (0, 1, -1, 2):
                arrive(wa(-1, dx), f"z1m{dx}")
                arrive(wa(1, dx), f"z1p{dx}")
        else:
            arrive(za(-s, c), f"z{s}m")
            arrive(za(s, c), f"z{s}p")
        if s < 3:
            same(za(-s, c), zp, f"z{s + 1}m")
            same(za(s, c), zm, f"z{s + 1}p")
        else:
            same(za(-s, c, 0, HX), zp, "z4m")
            same(za(s, c, HX, HX), zm, "z4p")
        same(za(-s, c), sib, f"sz{s}m")
        same(za(s, c), sib, f"sz{s}p")

    def a_last():
        arrive(za(4, c, 0, HX), "z4m")
        arrive(za(4, c, HX, HX), "z4p")
        same(za(4, c), sib, "sz4")

    def a_done():
        arrive(za(0, 1 - c), "sz0")
        for s in (1, 2, 3):
            arrive(za(-s, 1 - c), f"sz{s}m")
            arrive(za(s, 1 - c), f"sz{s}p")
        arrive(za(4, 1 - c), "sz4")

    def bx_piece(dz):
        same(bp(dz, 0), xp, f"x1m{dz}")
        same(bp(dz, 0), xm, f"x1p{dz}")

    def b_start():
        same(wb(0), zp, "b1m")
        same(wb(0), zm, "b1p")

    def b_step(s):
        arrive(wb(-s), f"b{s}m")
        arrive(wb(s), f"b{s}p")
        if s < 3:
            same(wb(-s), zp, f"b{s + 1}m")
            same(wb(s), zm, f"b{s + 1}p")
        else:
            same(wb(-s, LA, BH), zp, "b4m")
            same(wb(s, LA + BH, BH), zm, "b4p")
        bx_piece(-s)
        bx_piece(s)

    def b_turn():
        arrive(wb(4, LA, BH), "b4m")
        arrive(wb(4, LA + BH, BH), "b4p")
        bx_piece(4)
        same(xb(0, c), sib, "sx0")

    DOWN = (-1, -2, -3, 4)

    def b_cross(i):
        up, down = i, DOWN[i]
        arrive(bp(up, -1), f"x1m{up}")
        same(bp(up, -1), xp, f"x2m{up}")
        arrive(bp(down, 1), f"x1p{down}")
        same(bp(down, 1), xm, f"x2p{down}")
        same(bp(up, -1), sib, "sx1m")
        same(bp(down, 1), sib, "sx1p")

    def b_collect(i):
        up, down = i, DOWN[i]
        arrive(bp(down, -1), f"x1m{down}")
        arrive(bp(up, 1), f"x1p{up}")
        same(bp(down, -1), sib, "sx1m")
        same(bp(up, 1), sib, "sx1p")

    def b_last(i):
        up, down = i, DOWN[i]
        arrive(bp(up, 2), f"x2m{up}")
        arrive(bp(down, 2), f"x2p{down}")
        same(bp(up, 2), sib, "sx2")
        same(bp(down, 2), sib, "sx2")

    def b_done():
        arrive(xb(0, 1 - c), "sx0")
        arrive(xb(-1, 1 - c), "sx1m")
        arrive(xb(1, 1 - c), "sx1p")
        arrive(xb(2, 1 - c), "sx2")

    QR = ROWS // NY

    def quarter(slot, dy, lo=0, n=QR):
        return packs.at[slot, pl.ds(pl.multiple_of(wrap(y + dy, NY) * QR + lo, 16), n)]

    def spread(slot, tag):
        def one():
            arrive(quarter(slot, 0), tag)
            same(quarter(slot, 0), yp, tag + "1m")
            same(quarter(slot, 0), ym, tag + "1p")

        def two():
            arrive(quarter(slot, -1), tag + "1m")
            same(quarter(slot, -1, 0, QR // 2), yp, tag + "2m")
            arrive(quarter(slot, 1), tag + "1p")
            same(quarter(slot, 1, QR // 2, QR // 2), ym, tag + "2p")

        def three():
            arrive(quarter(slot, 2, 0, QR // 2), tag + "2m")
            arrive(quarter(slot, 2, QR // 2, QR // 2), tag + "2p")

        return one, two, three

    f_lat.wait()
    send(quarter(0, 0), quarter(2, 0), nextc, "l2")
    send(docs.at[0], docs.at[2], nextc, "d2")
    for d in f_w:
        d.wait()
    a_start()
    b_start()
    bx_piece(0)
    za_piece(0)

    @pl.when(c == 0)
    def _():
        copy_at(packs.at[0], packs.at[1], sib, "l1", S_ALT).start()
        copy_at(docs.at[0], docs.at[1], sib, "d1", S_ALT + 1).start()
        copy_at(docs.at[0], docs.at[3], nexto, "d3", S_ALT + 2).start()

    @pl.when(c == 1)
    def _():
        copy_at(docs.at[0], docs.at[1], nexto, "d1", S_ALT + 1).start()
        copy_at(docs.at[0], docs.at[3], chip(k + 2, 0), "d3", S_ALT + 2).start()

    send(gb_ref, gbs.at[y], yp, "gm")
    send(gb_ref, gbs.at[y], ym, "gp")
    send(gb_ref, gbs.at[y], yy, "g2")
    dcol[8 : 8 + ROWS, :] = jnp.broadcast_to(doc_column(0), (ROWS, 128))
    f_qr.wait()
    for t in range(4):
        v = turned(qraw[:, t * 128 : t * 128 + 128].astype(F32))
        qr[:, t * 256 : t * 256 + 128] = jnp.where(lane < ROPE, v, 0.0).astype(BF)
        qr[:, t * 256 + 128 : t * 256 + 256] = jnp.where(lane >= ROPE, v, 0.0).astype(BF)

    def attend(slot, back, kind, first=False, last=False):
        kdoc = jnp.where(sp >= back, docs[slot, 0:1, :], -1.0)
        ok = dcol[8 : 8 + ROWS, 0:1] == kdoc
        if kind == "diag":
            qi_pos = lax.broadcasted_iota(jnp.int32, (ROWS, ROWS), 0)
            ki_pos = lax.broadcasted_iota(jnp.int32, (ROWS, ROWS), 1)
            ok = ok & (ki_pos <= qi_pos)
        bias[...] = jnp.where(ok, 0.0, masked_score)
        ones = jnp.ones((ROWS, 128), BF)

        def body(group, carry):
            lat = packs[slot, :, 0:512]
            kr = packs[slot, :, 512:640]
            lanes, states, results = [], [], []
            for hh in range(GROUP):
                h = group * GROUP + hh
                lanes.append(pl.ds(pl.multiple_of(h * 128, 128), 128))
                if not first:
                    states.append((mrun[h], lrun[h], acc[h]))
            pairs = {}

            def keys(i):
                both = pl.ds(pl.multiple_of((group * GROUP + 2 * i) * 128, 256), 256)
                pairs[i] = (
                    (dot(lat, kup[:, both]) * SCALE2).astype(BF),
                    dot(lat, vup[:, both]).astype(BF),
                )

            def score(hh):
                k2 = pairs[hh // 2][0][:, hh % 2 * 128 : hh % 2 * 128 + 128]
                q = jnp.concatenate([qn[:, lanes[hh]], qr[:, lanes[hh]]], axis=1)
                return dot_nt(q, jnp.concatenate([k2, kr], axis=1)) + bias[...]

            keys(0)
            ahead = score(0)
            for hh in range(GROUP):
                s = ahead
                if hh % 2 == 0 and hh + 2 < GROUP:
                    keys(hh // 2 + 1)
                if hh + 1 < GROUP:
                    ahead = score(hh + 1)
                v2 = pairs[hh // 2][1][:, hh % 2 * 128 : hh % 2 * 128 + 128]
                mx = jnp.max(s, axis=1, keepdims=True)
                if first:
                    mnew = jnp.broadcast_to(mx, (ROWS, 128))
                else:
                    mnew = jnp.maximum(states[hh][0], mx)
                p = jnp.exp2(s - mnew[:, 0:1])
                o = dot(p.astype(BF), jnp.concatenate([v2, ones], axis=1))
                o, total = o[:, 0:128], o[:, 128:256]
                if not first:
                    alpha = jnp.exp2(states[hh][0] - mnew)
                    total = states[hh][1] * alpha + total
                    o = states[hh][2] * alpha + o
                results.append((mnew, total, o))
            for hh in range(GROUP):
                h = group * GROUP + hh
                mnew, total, o = results[hh]
                if last:
                    att[:, lanes[hh]] = (o / total).astype(BF)
                else:
                    mrun[h] = mnew
                    lrun[h] = total
                    acc[h] = o
            return carry

        lax.fori_loop(0, 8 // GROUP, body, 0)

    f_kup.wait()
    f_qn.wait()
    f_vup.wait()
    slot_two = spread(2, "l2")
    slot_three = spread(3, "l3")
    attend(0, 0, "diag", first=True)
    slot_two[0]()

    @pl.when(c == 1)
    def _():
        copy_at(quarter(2, 0), quarter(3, 0), nexto, "l3", S_ALT).start()

    a_one()
    slot_two[1]()
    b_step(1)
    slot_two[2]()

    @pl.when(c == 0)
    def _():
        copy_at(packs.at[2], packs.at[3], sib, "s3", S_ALT + 3).start()
        before = len(sends)
        slot_three[0]()
        for i in range(before, len(sends)):
            zero_only.append(i)
            sends[i] = None

    @pl.when(c == 1)
    def _():
        copy_at(packs.at[2], packs.at[1], sib, "l1", S_ALT + 3).start()

    arrive(docs.at[2], "d2")
    attend(2, 2, "full")
    a_two()
    b_step(2)
    b_cross(0)

    @pl.when(c == 0)
    def _():
        before = len(sends)
        slot_three[1]()
        for i in range(before, len(sends)):
            zero_only.append(i)
            sends[i] = None

    arrive(packs.at[1], "l1")
    arrive(docs.at[1], "d1")
    before = jnp.where(sp >= 1, doc_column(1)[ROWS - 8 : ROWS, :], -1.0)
    dcol[0:8, :] = jnp.broadcast_to(before, (8, 128))
    attend(1, 1, "full")
    a_step(1)
    arrive(docs.at[3], "d3")

    @pl.when(c == 0)
    def _():
        slot_three[2]()

    @pl.when(c == 1)
    def _():
        arrive(packs.at[3], "s3")

    attend(3, 3, "far", last=True)

    UP, LOW = pl.ds(0, HALF), pl.ds(HALF, HALF)

    def far_all(chunk, tag, ra):
        sa[...] = chunk(wrap(y + 2, NY), pl.ds(0, ROWS)).astype(BF)
        send(sa.at[UP], ra.at[0], yp, tag + "am")
        send(sa.at[LOW], ra.at[1], ym, tag + "ap")

    def near_all(chunk, tag, rb):
        f = chunk(wrap(y + 1, NY), pl.ds(0, ROWS))
        pfp[...] = f[:HALF]
        sp_buf[LOW, :] = f[HALF:].astype(BF)
        send(sp_buf.at[LOW], rb.at[0, LOW], yp, tag + "bm1")
        f = chunk(wrap(y - 1, NY), pl.ds(0, ROWS))
        pfm[...] = f[HALF:]
        sm_buf[UP, :] = f[:HALF].astype(BF)
        send(sm_buf.at[UP], rb.at[1, UP], ym, tag + "bp0")

    def forward(tag, ra, rb):
        arrive(ra.at[0], tag + "am")
        sp_buf[UP, :] = (pfp[...] + ra[0].astype(F32)).astype(BF)
        send(sp_buf.at[UP], rb.at[0, UP], yp, tag + "bm0")
        arrive(ra.at[1], tag + "ap")
        sm_buf[LOW, :] = (pfm[...] + ra[1].astype(F32)).astype(BF)
        send(sm_buf.at[LOW], rb.at[1, LOW], ym, tag + "bp1")

    def collected(tag, rb):
        arrive(rb.at[0, LOW], tag + "bm1")
        arrive(rb.at[1, UP], tag + "bp0")
        arrive(rb.at[0, UP], tag + "bm0")
        arrive(rb.at[1, LOW], tag + "bp1")
        return own[...] + rb[0].astype(F32) + rb[1].astype(F32)

    def settle(ds):
        for d in ds:
            d.wait_send()

    f_op.wait()
    f_res.wait()

    def head_share(t, rows):
        return dot(att[rows, :], op[:, pl.ds(pl.multiple_of(t * CH, CH), CH)])

    mark = len(sends)

    far_all(head_share, "p", ra)
    near_all(head_share, "p", rb)
    own[...] = head_share(y, pl.ds(0, ROWS))
    b_step(3)
    forward("p", ra, rb)
    b_turn()
    b_cross(1)
    b_cross(2)
    a_step(2)
    total_one = collected("p", rb)
    m4[y] = (residual_scale * res[...].astype(F32) + total_one).astype(BF)

    def piece(dy, lo):
        return m4.at[wrap(y + dy, NY), pl.ds(lo, HALF)]

    same(piece(0, 0), yp, "m1m0")
    same(piece(0, HALF), ym, "m1p1")
    same(piece(0, HALF), yp, "m1m1")
    same(piece(0, 0), ym, "m1p0")
    b_cross(3)
    arrive(piece(-1, 0), "m1m0")
    same(piece(-1, 0), yp, "m2m")
    arrive(piece(1, HALF), "m1p1")
    same(piece(1, HALF), ym, "m2p")
    arrive(gbs.at[wrap(y - 1, NY)], "gm")
    arrive(gbs.at[wrap(y + 1, NY)], "gp")
    arrive(gbs.at[wrap(y + 2, NY)], "g2")
    gbs[y] = gb_ref[...]
    a_step(3)
    for i in range(4):
        b_collect(i)
    arrive(piece(-1, HALF), "m1m1")
    arrive(piece(1, 0), "m1p0")
    for i in range(4):
        b_last(i)
    arrive(piece(2, 0), "m2m")
    arrive(piece(2, HALF), "m2p")

    def norm_of(src, rows, out_rows):
        parts = [src[t, rows, :].astype(F32) for t in range(NY)]
        s = sum(jnp.sum(v, axis=1, keepdims=True) for v in parts) / D
        q = sum(jnp.sum(v * v, axis=1, keepdims=True) for v in parts) / D
        r = lax.rsqrt(q - s * s + norm_eps)
        for t in range(NY):
            nf[out_rows, t * CH : (t + 1) * CH] = (
                (parts[t] - s) * r * gbs[t, 0:1, :] + gbs[t, 1:2, :]
            ).astype(BF)

    def norm_rows(i, carry):
        first = pl.multiple_of(i * 32, 32)
        norm_of(m4, pl.ds(first, 32), pl.ds(pl.multiple_of(first + LEAD, 16), 32))
        return carry

    tail = m4.at[:, pl.ds(ROWS - LEAD, LEAD), :]
    copy_to(tail, before_rows, sib, "t")
    tail_at = len(sends) - 1

    @pl.when(c == 0)
    def _():
        copy_at(tail, before_rows, sib, "t", tail_at).start()

    @pl.when(c == 1)
    def _():
        copy_at(tail, before_rows, nexto, "t", tail_at).start()

    a_last()
    lax.fori_loop(0, ROWS // 32, norm_rows, 0)
    b_done()
    a_done()

    arrive(before_rows, "t")
    norm_of(before_rows, pl.ds(0, LEAD), pl.ds(0, LEAD))
    for d in f_taps:
        d.wait()

    def block(base, j):
        return pl.ds(pl.multiple_of(base + j * 128, 128), 128)

    KC = D // PARTS
    RC = ROWS // PARTS

    def up_part(j, i):
        zs = slice(i * NZ // PARTS, (i + 1) * NZ // PARTS)
        both = jnp.concatenate(
            [w[zs, :, :, :, block(DA, j)], w[zs, :, :, :, block(LA, j)]], axis=4
        )
        return dot(nf[:, i * KC : (i + 1) * KC], both.reshape(KC, 256))

    def keep(j, f):
        gv[:, block(0, j)] = f[:, 0:128]
        gv[:, block(UNITS, j)] = f[:, 128:256]

    def conv_part(j, i):
        r0 = i * RC
        here = dcol[8 + r0 : 8 + r0 + RC, :]
        near = (dcol[7 + r0 : 7 + r0 + RC, :] == here).astype(F32)
        far = (dcol[6 + r0 : 6 + r0 + RC, :] == here).astype(F32)

        def mix(taps, base):
            lo = LEAD + r0
            a0 = gv[lo - 2 : lo - 2 + RC, block(base, j)]
            a1 = gv[lo - 1 : lo - 1 + RC, block(base, j)]
            a2 = gv[lo : lo + RC, block(base, j)]
            t = taps[:, block(0, j)].astype(F32)
            return t[0:1] * a0 * far + t[1:2] * a1 * near + t[2:3] * a2

        g = mix(cg_ref, 0)
        v = mix(cv_ref, UNITS)
        act = 0.5 * g * (1.0 + jnp.tanh(0.7978845608028654 * (g + 0.044715 * (g * g * g))))
        return (v * act).astype(BF)

    def step(j, carry):
        f, done = None, []
        for i in range(PARTS):
            part = up_part(j, i)
            f = part if f is None else f + part
            done.append(conv_part(j - 1, i))
        for i in range(PARTS):
            hid[i * RC : (i + 1) * RC, block(0, j - 1)] = done[i]
        keep(j, f)
        return carry

    f = up_part(0, 0)
    for i in range(1, PARTS):
        f = f + up_part(0, i)
    keep(0, f)
    lax.fori_loop(1, UNITS // 128, step, 0)
    for i in range(PARTS):
        hid[i * RC : (i + 1) * RC, block(0, UNITS // 128 - 1)] = conv_part(UNITS // 128 - 1, i)

    def unit_share(t, rows):
        part = pl.ds(2 * t, 2)
        da = w[part, :, :, :, 0:DA].reshape(CH, DA)
        db = w[part, :, :, :, LA + UNITS : LW].reshape(CH, UNITS - DA)
        return dot_nt(hid[rows, 0:DA], da) + dot_nt(hid[rows, DA:UNITS], db)

    settle(sends[mark : mark + 6])
    early = len(sends)

    def settle_early():
        settle(d for d in sends[:mark] if d is not None)
        settle(sends[mark + 6 : early])
        copy_at(docs.at[0], docs.at[1], sib, "d1", S_ALT + 1).wait_send()
        copy_at(docs.at[0], docs.at[3], sib, "d3", S_ALT + 2).wait_send()
        copy_at(packs.at[2], packs.at[3], sib, "s3", S_ALT + 3).wait_send()

        @pl.when(c == 0)
        def _():
            copy_at(packs.at[0], packs.at[1], sib, "l1", S_ALT).wait_send()
            for i, at in enumerate(zero_only):
                part = quarter(3, 0, 0, QR if i < 2 else QR // 2)
                copy_at(part, part, yp, "l3", at).wait_send()

        @pl.when(c == 1)
        def _():
            copy_at(quarter(2, 0), quarter(3, 0), nexto, "l3", S_ALT).wait_send()

    far_all(unit_share, "u", ra2)
    near_all(unit_share, "u", rb2)
    own[...] = unit_share(y, pl.ds(0, ROWS))
    settle_early()
    forward("u", ra2, rb2)
    total_two = collected("u", rb2)
    mixed = (
        residual_scale * nf[LEAD : LEAD + ROWS, pl.ds(pl.multiple_of(y * CH, CH), CH)].astype(F32) + total_two
    )
    own[...] = mixed
    s = jnp.sum(mixed, axis=1, keepdims=True)
    q = jnp.sum(mixed * mixed, axis=1, keepdims=True)
    both = jnp.where(lane == 0, s, jnp.where(lane == 1, q, 0.0))
    stats[y] = both.T[0:8, :]
    same(stats.at[y], yp, "qm")
    same(stats.at[y], ym, "qp")
    same(stats.at[y], yy, "q2")
    settle(sends[early:])
    arrive(stats.at[wrap(y - 1, NY)], "qm")
    arrive(stats.at[wrap(y + 1, NY)], "qp")
    arrive(stats.at[wrap(y + 2, NY)], "q2")
    tot = (stats[0] + stats[1]) + (stats[2] + stats[3])
    back = jnp.concatenate([tot, jnp.zeros((120, ROWS), F32)], axis=0).T
    s = back[:, 0:1] / D
    q = back[:, 1:2] / D
    r = lax.rsqrt(q - s * s + norm_eps)
    out_ref[...] = ((own[...] - s) * r * gb_ref[2:3, :] + gb_ref[3:4, :]).astype(BF)


def local(
    residual, query_nope, query_rope, latent, rope_key, doc_ids, key_up, value_up, out_proj,
    norm1_gain, norm1_bias, ffn_gate, ffn_value, conv_gate, conv_value, ffn_down,
    norm2_gain, norm2_bias,
):
    rows = latent.shape[0]
    turn = rope_base_freq ** (-np.arange(0, ROPE, 2, dtype=np.float64) / ROPE)
    turn = jnp.asarray(np.tile(np.tile(turn, 4)[None], (8, 1)).astype(np.float32))

    anyspec = pl.BlockSpec(memory_space=pl.ANY)
    vspec = pl.BlockSpec(memory_space=pltpu.VMEM)
    V = pltpu.VMEM
    return pl.pallas_call(
        layer_kernel,
        out_shape=jax.ShapeDtypeStruct((rows, CH), BF),
        in_specs=[anyspec] * 19,
        out_specs=vspec,
        scratch_shapes=[
            V((ROPE, ROWS), BF),
            V((CH,), BF),
            V((CH,), BF),
            V((CH,), BF),
            V((CH,), BF),
            V((ROWS,), jnp.int32),
            V((CONV, UNITS), BF),
            V((CONV, UNITS), BF),
            V((8, 128), F32),
            V((8, CH), F32),
            V((ROWS, 128), F32),
            V((ROWS, 128), F32),
            V((4, ROWS, PACKW), BF),
            V((ROWS, 1024), BF),
            V((ROWS, CH), BF),
            V((ROWS, 1024), BF),
            V((512, 1024), BF),
            V((512, 1024), BF),
            V((1024, D), BF),
            V((ROWS, CH), BF),
            V((NZ, NX, 2, 32, LW), BF),
            V((NY, 8, CH), F32),
            V((ROWS, 1024), BF),
            V((8, ROWS, 128), F32),
            V((8, ROWS, 128), F32),
            V((8, ROWS, 128), F32),
            V((8 + ROWS, 128), F32),
            V((4, 8, ROWS), F32),
            V((ROWS, ROWS), F32),
            V((ROWS, CH), BF),
            V((ROWS, CH), BF),
            V((ROWS, CH), BF),
            V((HALF, CH), F32),
            V((HALF, CH), F32),
            V((ROWS, CH), F32),
            V((2, HALF, CH), BF),
            V((2, ROWS, CH), BF),
            V((2, HALF, CH), BF),
            V((2, ROWS, CH), BF),
            V((NY, ROWS, CH), BF),
            V((LEAD + ROWS, D), BF),
            V((LEAD + ROWS, 2 * UNITS), F32),
            V((ROWS, UNITS), BF),
            V((NY, LEAD, CH), BF),
            V((NY, 8, ROWS), F32),
            pltpu.SemaphoreType.DMA((24,)),
            pltpu.SemaphoreType.DMA((N_SEND,)),
            pltpu.SemaphoreType.DMA((N_RECV,)),
        ],
        compiler_params=pltpu.CompilerParams(
            collective_id=0, has_side_effects=True, vmem_limit_bytes=54 * 1024 * 1024
        ),
    )(
        latent, query_nope, query_rope, key_up, value_up, out_proj, residual,
        ffn_gate, ffn_value, ffn_down.T, rope_key.T, norm1_gain, norm1_bias, norm2_gain, norm2_bias,
        doc_ids, conv_gate, conv_value, turn,
    )


def solution(mesh):
    placed = (
        P("sp", "tp"),
        P("sp", "tp"),
        P("sp", "tp"),
        P("sp", None),
        P("sp", None),
        P("sp"),
        P(None, "tp"),
        P(None, "tp"),
        P("tp", None),
        P("tp"),
        P("tp"),
        P("sp", "tp"),
        P("sp", "tp"),
        P(None, "tp"),
        P(None, "tp"),
        P("tp", "sp"),
        P("tp"),
        P("tp"),
    )
    return jax.shard_map(
        local, mesh=mesh, in_specs=placed, out_specs=P("sp", "tp"), check_vma=False
    )
```

```python
import jax
import jax.numpy as jnp
import numpy as np
from jax import lax
from jax.experimental import pallas as pl
from jax.experimental.pallas import tpu as pltpu
from jax.sharding import PartitionSpec as P

D = 2048
NOPE = 128
ROPE = 64
VDIM = 128
CONV = 3
REACH = 3

norm_eps = 1e-05
residual_scale = 8.0**0.25
rope_base_freq = 10000.0
masked_score = -1e30
SCALE2 = (NOPE + ROPE) ** (-0.5) * 1.4426950408889634

NX, NZ, NY = 4, 8, 4
ROWS = 384
HALF = ROWS // 2
LEAD = 16
PARTS = 4
CH = 512
UNITS = 1408
DA = 256
LA = DA + UNITS
LW = 3 * UNITS
PACKW = 640
GROUP = 8
N_SEND = 128
N_RECV = 128
S_ALT = N_SEND - 4
MESH = pl.DeviceIdType.MESH
BF = jnp.bfloat16
F32 = jnp.float32


def dot(a, b):
    return jnp.dot(a, b, preferred_element_type=F32)


def dot_nt(a, b):
    return lax.dot_general(a, b, (((1,), (1,)), ((), ())), preferred_element_type=F32)


def layer_kernel(
    lat_h, qn_h, qr_h, kup_h, vup_h, op_h, res_h, gate_h, value_h, down_h,
    key_h, g1_h, b1_h, g2_h, b2_h, doc_h, cg_h, cv_h, freq_h,
    out_ref,
    key_ref, v0, v1, v2, v3, doc_ref, cg_ref, cv_ref, freq_ref, gb_ref, cos_ref, sin_ref,
    packs, qn, qraw, qr, kup, vup, op, res, w, gbs, att, acc, mrun, lrun, dcol, docs, bias,
    sa, sp_buf, sm_buf, pfp, pfm, own, ra, rb, ra2, rb2, m4, nf, gv, hid, before_rows, stats,
    lsem, ssem, rsem,
):
    sp = lax.axis_index("sp")
    y = lax.axis_index("tp")
    c = lax.rem(sp, 2)
    k = lax.div(sp, 2)
    x = lax.rem(k, NX)
    z = lax.div(k, NX)

    def wrap(v, n):
        return lax.rem(v + n, n)

    def dev(zz, xx, cc, yy):
        return ((wrap(zz, NZ) * NX + wrap(xx, NX)) * 2 + cc, wrap(yy, NY))

    def chip(kk, cc):
        return (wrap(kk, NZ * NX) * 2 + cc, y)

    xp, xm = dev(z, x + 1, c, y), dev(z, x - 1, c, y)
    zp, zm = dev(z + 1, x, c, y), dev(z - 1, x, c, y)
    sib = dev(z, x, 1 - c, y)
    yp, ym, yy = dev(z, x, c, y + 1), dev(z, x, c, y - 1), dev(z, x, c, y + 2)
    nextc, prevc = chip(k + 1, c), chip(k - 1, c)
    nexto, prevo = chip(k + 1, 1 - c), chip(k - 1, 1 - c)

    local = []
    def fetch(src, dst):
        d = pltpu.make_async_copy(src, dst, lsem.at[len(local)])
        d.start()
        local.append(d)
        return d
    f_small = [
        fetch(key_h, key_ref),
        fetch(freq_h, freq_ref),
        fetch(doc_h, doc_ref),
        fetch(g1_h, v0),
        fetch(b1_h, v1),
        fetch(g2_h, v2),
        fetch(b2_h, v3),
    ]
    f_lat = fetch(lat_h, packs.at[0, :, pl.ds(0, 512)])
    mine = w.at[z, x, c]
    f_w = [
        fetch(gate_h, mine.at[:, pl.ds(DA, UNITS)]),
        fetch(value_h, mine.at[:, pl.ds(LA, UNITS)]),
        fetch(down_h.at[:, pl.ds(0, DA)], mine.at[:, pl.ds(0, DA)]),
        fetch(down_h.at[:, pl.ds(DA, UNITS - DA)], mine.at[:, pl.ds(LA + UNITS, UNITS - DA)]),
    ]
    f_qr = fetch(qr_h, qraw)
    f_kup = fetch(kup_h, kup)
    f_qn = fetch(qn_h, qn)
    f_vup = fetch(vup_h, vup)
    f_taps = [fetch(cg_h, cg_ref), fetch(cv_h, cv_ref)]
    f_op = fetch(op_h, op)
    f_res = fetch(res_h, res)

    barrier = pltpu.get_barrier_semaphore()
    peers = (
        xp, xm, zp, zm, sib, yp, ym, yy, nextc, prevc, nexto, prevo,
        chip(k + 2, 1 - c), chip(k - 2, 1 - c),
    )
    for p in peers:
        pl.semaphore_signal(barrier, inc=1, device_id=p, device_id_type=MESH)
    lane = lax.broadcasted_iota(jnp.int32, (ROWS, 128), 1)
    front = lax.rem(lane, ROPE) < ROPE // 2

    def turned(v):
        swapped = jnp.where(front, pltpu.roll(v, 128 - ROPE // 2, 1), pltpu.roll(v, ROPE // 2, 1))
        return v * cos_ref[...] + swapped * sin_ref[...]

    for d in f_small:
        d.wait()
    place = lax.broadcasted_iota(jnp.int32, (ROWS, 128), 0) + sp * ROWS
    angle = place.astype(F32) * freq_ref[0:1, :]
    cos_ref[...] = jnp.cos(angle)
    sin_ref[...] = jnp.where(front, -1.0, 1.0) * jnp.sin(angle)
    key = key_ref[...].astype(F32)
    packs[0, :, 512:640] = (turned(jnp.concatenate([key, key], axis=0).T) * SCALE2).astype(BF)
    docs[0] = jnp.broadcast_to(doc_ref[...].astype(F32).reshape(1, ROWS), (8, ROWS))
    gb_ref[...] = jnp.concatenate(
        [v[...].astype(F32).reshape(1, CH) for v in (v0, v1, v2, v3)] + [jnp.zeros((4, CH), F32)], axis=0
    )
    def doc_column(slot):
        return jnp.concatenate([docs[slot], jnp.zeros((120, ROWS), F32)], axis=0).T[:, 0:1]

    pl.semaphore_wait(barrier, len(peers))

    sends = []
    zero_only = []
    names = {}

    def rid(name):
        return names.setdefault(name, len(names))

    def copy_to(src, dst, to, name):
        d = pltpu.make_async_remote_copy(
            src_ref=src, dst_ref=dst, send_sem=ssem.at[len(sends)],
            recv_sem=rsem.at[rid(name)], device_id=to, device_id_type=MESH,
        )
        sends.append(d)
        return d

    def copy_at(src, dst, to, name, at):
        return pltpu.make_async_remote_copy(
            src_ref=src, dst_ref=dst, send_sem=ssem.at[at],
            recv_sem=rsem.at[rid(name)], device_id=to, device_id_type=MESH,
        )

    def send(src, dst, to, name):
        copy_to(src, dst, to, name).start()

    def arrive(dst, name):
        pltpu.make_async_remote_copy(
            src_ref=dst, dst_ref=dst, send_sem=ssem.at[0],
            recv_sem=rsem.at[rid(name)], device_id=sib, device_id_type=MESH,
        ).wait_recv()

    def wa(dz, dx):
        return w.at[wrap(z + dz, NZ), wrap(x + dx, NX), c, :, pl.ds(0, LA)]

    def za(dz, cc, lo=0, n=NX):
        return w.at[wrap(z + dz, NZ), pl.ds(lo, n), cc, :, pl.ds(0, LA)]

    def wb(dz, lo=LA, n=LW - LA):
        return w.at[wrap(z + dz, NZ), x, c, :, pl.ds(lo, n)]

    def xb(dx, cc, lo=0, n=NZ):
        return w.at[pl.ds(lo, n), wrap(x + dx, NX), cc, :, pl.ds(LA, LW - LA)]

    BH = (LW - LA) // 2
    HX = NX // 2

    def bp(dz, dx):
        return w.at[wrap(z + dz, NZ), wrap(x + dx, NX), c, :, pl.ds(LA, LW - LA)]

    def same(ref, to, name):
        send(ref, ref, to, name)

    def a_start():
        same(wa(0, 0), xp, "a1m")
        same(wa(0, 0), xm, "a1p")

    def za_piece(dx):
        same(wa(0, dx), zp, f"z1m{dx}")
        same(wa(0, dx), zm, f"z1p{dx}")

    def a_one():
        arrive(wa(0, 1), "a1p")
        same(wa(0, 1), xm, "a2p")
        za_piece(1)

    def a_two():
        arrive(wa(0, -1), "a1m")
        za_piece(-1)
        arrive(wa(0, 2), "a2p")
        za_piece(2)
        same(za(0, c), sib, "sz0")

    def a_step(s):
        if s == 1:
            for dx in (0, 1, -1, 2):
                arrive(wa(-1, dx), f"z1m{dx}")
                arrive(wa(1, dx), f"z1p{dx}")
        else:
            arrive(za(-s, c), f"z{s}m")
            arrive(za(s, c), f"z{s}p")
        if s < 3:
            same(za(-s, c), zp, f"z{s + 1}m")
            same(za(s, c), zm, f"z{s + 1}p")
        else:
            same(za(-s, c, 0, HX), zp, "z4m")
            same(za(s, c, HX, HX), zm, "z4p")
        same(za(-s, c), sib, f"sz{s}m")
        same(za(s, c), sib, f"sz{s}p")

    def a_last():
        arrive(za(4, c, 0, HX), "z4m")
        arrive(za(4, c, HX, HX), "z4p")
        same(za(4, c), sib, "sz4")

    def a_done():
        arrive(za(0, 1 - c), "sz0")
        for s in (1, 2, 3):
            arrive(za(-s, 1 - c), f"sz{s}m")
            arrive(za(s, 1 - c), f"sz{s}p")
        arrive(za(4, 1 - c), "sz4")

    def bx_piece(dz):
        same(bp(dz, 0), xp, f"x1m{dz}")
        same(bp(dz, 0), xm, f"x1p{dz}")

    def b_start():
        same(wb(0), zp, "b1m")
        same(wb(0), zm, "b1p")

    def b_step(s):
        arrive(wb(-s), f"b{s}m")
        arrive(wb(s), f"b{s}p")
        if s < 3:
            same(wb(-s), zp, f"b{s + 1}m")
            same(wb(s), zm, f"b{s + 1}p")
        else:
            same(wb(-s, LA, BH), zp, "b4m")
            same(wb(s, LA + BH, BH), zm, "b4p")
        bx_piece(-s)
        bx_piece(s)

    def b_turn():
        arrive(wb(4, LA, BH), "b4m")
        arrive(wb(4, LA + BH, BH), "b4p")
        bx_piece(4)
        same(xb(0, c), sib, "sx0")

    DOWN = (-1, -2, -3, 4)

    def b_cross(i):
        up, down = i, DOWN[i]
        arrive(bp(up, -1), f"x1m{up}")
        same(bp(up, -1), xp, f"x2m{up}")
        arrive(bp(down, 1), f"x1p{down}")
        same(bp(down, 1), xm, f"x2p{down}")
        same(bp(up, -1), sib, "sx1m")
        same(bp(down, 1), sib, "sx1p")

    def b_collect(i):
        up, down = i, DOWN[i]
        arrive(bp(down, -1), f"x1m{down}")
        arrive(bp(up, 1), f"x1p{up}")
        same(bp(down, -1), sib, "sx1m")
        same(bp(up, 1), sib, "sx1p")

    def b_last(i):
        up, down = i, DOWN[i]
        arrive(bp(up, 2), f"x2m{up}")
        arrive(bp(down, 2), f"x2p{down}")
        same(bp(up, 2), sib, "sx2")
        same(bp(down, 2), sib, "sx2")

    def b_done():
        arrive(xb(0, 1 - c), "sx0")
        arrive(xb(-1, 1 - c), "sx1m")
        arrive(xb(1, 1 - c), "sx1p")
        arrive(xb(2, 1 - c), "sx2")

    QR = ROWS // NY

    def quarter(slot, dy, lo=0, n=QR):
        return packs.at[slot, pl.ds(pl.multiple_of(wrap(y + dy, NY) * QR + lo, 16), n)]

    def spread(slot, tag):
        def one():
            arrive(quarter(slot, 0), tag)
            same(quarter(slot, 0), yp, tag + "1m")
            same(quarter(slot, 0), ym, tag + "1p")

        def two():
            arrive(quarter(slot, -1), tag + "1m")
            same(quarter(slot, -1, 0, QR // 2), yp, tag + "2m")
            arrive(quarter(slot, 1), tag + "1p")
            same(quarter(slot, 1, QR // 2, QR // 2), ym, tag + "2p")

        def three():
            arrive(quarter(slot, 2, 0, QR // 2), tag + "2m")
            arrive(quarter(slot, 2, QR // 2, QR // 2), tag + "2p")

        return one, two, three

    f_lat.wait()
    send(quarter(0, 0), quarter(2, 0), nextc, "l2")
    send(docs.at[0], docs.at[2], nextc, "d2")
    for d in f_w:
        d.wait()
    a_start()
    b_start()
    bx_piece(0)
    za_piece(0)

    @pl.when(c == 0)
    def _():
        copy_at(packs.at[0], packs.at[1], sib, "l1", S_ALT).start()
        copy_at(docs.at[0], docs.at[1], sib, "d1", S_ALT + 1).start()
        copy_at(docs.at[0], docs.at[3], nexto, "d3", S_ALT + 2).start()

    @pl.when(c == 1)
    def _():
        copy_at(docs.at[0], docs.at[1], nexto, "d1", S_ALT + 1).start()
        copy_at(docs.at[0], docs.at[3], chip(k + 2, 0), "d3", S_ALT + 2).start()

    send(gb_ref, gbs.at[y], yp, "gm")
    send(gb_ref, gbs.at[y], ym, "gp")
    send(gb_ref, gbs.at[y], yy, "g2")
    dcol[8 : 8 + ROWS, :] = jnp.broadcast_to(doc_column(0), (ROWS, 128))
    f_qr.wait()
    for t in range(4):
        v = turned(qraw[:, t * 128 : t * 128 + 128].astype(F32))
        qr[:, t * 256 : t * 256 + 128] = jnp.where(lane < ROPE, v, 0.0).astype(BF)
        qr[:, t * 256 + 128 : t * 256 + 256] = jnp.where(lane >= ROPE, v, 0.0).astype(BF)

    def attend(slot, back, kind, first=False, last=False):
        kdoc = jnp.where(sp >= back, docs[slot, 0:1, :], -1.0)
        ok = dcol[8 : 8 + ROWS, 0:1] == kdoc
        if kind == "diag":
            qi_pos = lax.broadcasted_iota(jnp.int32, (ROWS, ROWS), 0)
            ki_pos = lax.broadcasted_iota(jnp.int32, (ROWS, ROWS), 1)
            ok = ok & (ki_pos <= qi_pos)
        bias[...] = jnp.where(ok, 0.0, masked_score)
        ones = jnp.ones((ROWS, 128), BF)

        def body(group, carry):
            lat = packs[slot, :, 0:512]
            kr = packs[slot, :, 512:640]
            lanes, states, results = [], [], []
            for hh in range(GROUP):
                h = group * GROUP + hh
                lanes.append(pl.ds(pl.multiple_of(h * 128, 128), 128))
                if not first:
                    states.append((mrun[h], lrun[h], acc[h]))
            pairs = {}

            def keys(i):
                both = pl.ds(pl.multiple_of((group * GROUP + 2 * i) * 128, 256), 256)
                pairs[i] = (
                    (dot(lat, kup[:, both]) * SCALE2).astype(BF),
                    dot(lat, vup[:, both]).astype(BF),
                )

            def score(hh):
                k2 = pairs[hh // 2][0][:, hh % 2 * 128 : hh % 2 * 128 + 128]
                q = jnp.concatenate([qn[:, lanes[hh]], qr[:, lanes[hh]]], axis=1)
                return dot_nt(q, jnp.concatenate([k2, kr], axis=1)) + bias[...]

            keys(0)
            ahead = score(0)
            for hh in range(GROUP):
                s = ahead
                if hh % 2 == 0 and hh + 2 < GROUP:
                    keys(hh // 2 + 1)
                if hh + 1 < GROUP:
                    ahead = score(hh + 1)
                v2 = pairs[hh // 2][1][:, hh % 2 * 128 : hh % 2 * 128 + 128]
                mx = jnp.max(s, axis=1, keepdims=True)
                if first:
                    mnew = jnp.broadcast_to(mx, (ROWS, 128))
                else:
                    mnew = jnp.maximum(states[hh][0], mx)
                p = jnp.exp2(s - mnew[:, 0:1])
                o = dot(p.astype(BF), jnp.concatenate([v2, ones], axis=1))
                o, total = o[:, 0:128], o[:, 128:256]
                if not first:
                    alpha = jnp.exp2(states[hh][0] - mnew)
                    total = states[hh][1] * alpha + total
                    o = states[hh][2] * alpha + o
                results.append((mnew, total, o))
            for hh in range(GROUP):
                h = group * GROUP + hh
                mnew, total, o = results[hh]
                if last:
                    att[:, lanes[hh]] = (o / total).astype(BF)
                else:
                    mrun[h] = mnew
                    lrun[h] = total
                    acc[h] = o
            return carry

        lax.fori_loop(0, 8 // GROUP, body, 0)

    f_kup.wait()
    f_qn.wait()
    f_vup.wait()
    slot_two = spread(2, "l2")
    slot_three = spread(3, "l3")
    attend(0, 0, "diag", first=True)
    slot_two[0]()

    @pl.when(c == 1)
    def _():
        copy_at(quarter(2, 0), quarter(3, 0), nexto, "l3", S_ALT).start()

    a_one()
    slot_two[1]()
    b_step(1)
    slot_two[2]()

    @pl.when(c == 0)
    def _():
        copy_at(packs.at[2], packs.at[3], sib, "s3", S_ALT + 3).start()
        before = len(sends)
        slot_three[0]()
        for i in range(before, len(sends)):
            zero_only.append(i)
            sends[i] = None

    @pl.when(c == 1)
    def _():
        copy_at(packs.at[2], packs.at[1], sib, "l1", S_ALT + 3).start()

    arrive(docs.at[2], "d2")
    attend(2, 2, "full")
    a_two()
    b_step(2)
    b_cross(0)

    @pl.when(c == 0)
    def _():
        before = len(sends)
        slot_three[1]()
        for i in range(before, len(sends)):
            zero_only.append(i)
            sends[i] = None

    arrive(packs.at[1], "l1")
    arrive(docs.at[1], "d1")
    before = jnp.where(sp >= 1, doc_column(1)[ROWS - 8 : ROWS, :], -1.0)
    dcol[0:8, :] = jnp.broadcast_to(before, (8, 128))
    attend(1, 1, "full")
    a_step(1)
    arrive(docs.at[3], "d3")

    @pl.when(c == 0)
    def _():
        slot_three[2]()

    @pl.when(c == 1)
    def _():
        arrive(packs.at[3], "s3")

    attend(3, 3, "far", last=True)

    UP, LOW = pl.ds(0, HALF), pl.ds(HALF, HALF)

    def far_all(chunk, tag, ra):
        sa[...] = chunk(wrap(y + 2, NY), pl.ds(0, ROWS)).astype(BF)
        send(sa.at[UP], ra.at[0], yp, tag + "am")
        send(sa.at[LOW], ra.at[1], ym, tag + "ap")

    def near_all(chunk, tag, rb):
        f = chunk(wrap(y + 1, NY), pl.ds(0, ROWS))
        pfp[...] = f[:HALF]
        sp_buf[LOW, :] = f[HALF:].astype(BF)
        send(sp_buf.at[LOW], rb.at[0, LOW], yp, tag + "bm1")
        f = chunk(wrap(y - 1, NY), pl.ds(0, ROWS))
        pfm[...] = f[HALF:]
        sm_buf[UP, :] = f[:HALF].astype(BF)
        send(sm_buf.at[UP], rb.at[1, UP], ym, tag + "bp0")

    def forward(tag, ra, rb):
        arrive(ra.at[0], tag + "am")
        sp_buf[UP, :] = (pfp[...] + ra[0].astype(F32)).astype(BF)
        send(sp_buf.at[UP], rb.at[0, UP], yp, tag + "bm0")
        arrive(ra.at[1], tag + "ap")
        sm_buf[LOW, :] = (pfm[...] + ra[1].astype(F32)).astype(BF)
        send(sm_buf.at[LOW], rb.at[1, LOW], ym, tag + "bp1")

    def collected(tag, rb):
        arrive(rb.at[0, LOW], tag + "bm1")
        arrive(rb.at[1, UP], tag + "bp0")
        arrive(rb.at[0, UP], tag + "bm0")
        arrive(rb.at[1, LOW], tag + "bp1")
        return own[...] + rb[0].astype(F32) + rb[1].astype(F32)

    def settle(ds):
        for d in ds:
            d.wait_send()

    f_op.wait()
    f_res.wait()

    def head_share(t, rows):
        return dot(att[rows, :], op[:, pl.ds(pl.multiple_of(t * CH, CH), CH)])

    mark = len(sends)

    far_all(head_share, "p", ra)
    near_all(head_share, "p", rb)
    own[...] = head_share(y, pl.ds(0, ROWS))
    b_step(3)
    forward("p", ra, rb)
    b_turn()
    b_cross(1)
    b_cross(2)
    a_step(2)
    total_one = collected("p", rb)
    m4[y] = (residual_scale * res[...].astype(F32) + total_one).astype(BF)

    def piece(dy, lo):
        return m4.at[wrap(y + dy, NY), pl.ds(lo, HALF)]

    same(piece(0, 0), yp, "m1m0")
    same(piece(0, HALF), ym, "m1p1")
    same(piece(0, HALF), yp, "m1m1")
    same(piece(0, 0), ym, "m1p0")
    b_cross(3)
    arrive(piece(-1, 0), "m1m0")
    same(piece(-1, 0), yp, "m2m")
    arrive(piece(1, HALF), "m1p1")
    same(piece(1, HALF), ym, "m2p")
    arrive(gbs.at[wrap(y - 1, NY)], "gm")
    arrive(gbs.at[wrap(y + 1, NY)], "gp")
    arrive(gbs.at[wrap(y + 2, NY)], "g2")
    gbs[y] = gb_ref[...]
    a_step(3)
    for i in range(4):
        b_collect(i)
    arrive(piece(-1, HALF), "m1m1")
    arrive(piece(1, 0), "m1p0")
    for i in range(4):
        b_last(i)
    arrive(piece(2, 0), "m2m")
    arrive(piece(2, HALF), "m2p")

    def norm_of(src, rows, out_rows):
        parts = [src[t, rows, :].astype(F32) for t in range(NY)]
        s = sum(jnp.sum(v, axis=1, keepdims=True) for v in parts) / D
        q = sum(jnp.sum(v * v, axis=1, keepdims=True) for v in parts) / D
        r = lax.rsqrt(q - s * s + norm_eps)
        for t in range(NY):
            nf[out_rows, t * CH : (t + 1) * CH] = (
                (parts[t] - s) * r * gbs[t, 0:1, :] + gbs[t, 1:2, :]
            ).astype(BF)

    def norm_rows(i, carry):
        first = pl.multiple_of(i * 32, 32)
        norm_of(m4, pl.ds(first, 32), pl.ds(pl.multiple_of(first + LEAD, 16), 32))
        return carry

    tail = m4.at[:, pl.ds(ROWS - LEAD, LEAD), :]
    copy_to(tail, before_rows, sib, "t")
    tail_at = len(sends) - 1

    @pl.when(c == 0)
    def _():
        copy_at(tail, before_rows, sib, "t", tail_at).start()

    @pl.when(c == 1)
    def _():
        copy_at(tail, before_rows, nexto, "t", tail_at).start()

    lax.fori_loop(0, ROWS // 32, norm_rows, 0)
    a_last()
    b_done()
    a_done()

    arrive(before_rows, "t")
    norm_of(before_rows, pl.ds(0, LEAD), pl.ds(0, LEAD))
    for d in f_taps:
        d.wait()

    def block(base, j):
        return pl.ds(pl.multiple_of(base + j * 128, 128), 128)

    KC = D // PARTS
    RC = ROWS // PARTS

    def up_part(j, i):
        zs = slice(i * NZ // PARTS, (i + 1) * NZ // PARTS)
        both = jnp.concatenate(
            [w[zs, :, :, :, block(DA, j)], w[zs, :, :, :, block(LA, j)]], axis=4
        )
        return dot(nf[:, i * KC : (i + 1) * KC], both.reshape(KC, 256))

    def keep(j, f):
        gv[:, block(0, j)] = f[:, 0:128]
        gv[:, block(UNITS, j)] = f[:, 128:256]

    def conv_part(j, i):
        r0 = i * RC
        here = dcol[8 + r0 : 8 + r0 + RC, :]
        near = (dcol[7 + r0 : 7 + r0 + RC, :] == here).astype(F32)
        far = (dcol[6 + r0 : 6 + r0 + RC, :] == here).astype(F32)

        def mix(taps, base):
            lo = LEAD + r0
            a0 = gv[lo - 2 : lo - 2 + RC, block(base, j)]
            a1 = gv[lo - 1 : lo - 1 + RC, block(base, j)]
            a2 = gv[lo : lo + RC, block(base, j)]
            t = taps[:, block(0, j)].astype(F32)
            return t[0:1] * a0 * far + t[1:2] * a1 * near + t[2:3] * a2

        g = mix(cg_ref, 0)
        v = mix(cv_ref, UNITS)
        act = 0.5 * g * (1.0 + jnp.tanh(0.7978845608028654 * (g + 0.044715 * (g * g * g))))
        return (v * act).astype(BF)

    def step(j, carry):
        f, done = None, []
        for i in range(PARTS):
            part = up_part(j, i)
            f = part if f is None else f + part
            done.append(conv_part(j - 1, i))
        for i in range(PARTS):
            hid[i * RC : (i + 1) * RC, block(0, j - 1)] = done[i]
        keep(j, f)
        return carry

    f = up_part(0, 0)
    for i in range(1, PARTS):
        f = f + up_part(0, i)
    keep(0, f)
    lax.fori_loop(1, UNITS // 128, step, 0)
    for i in range(PARTS):
        hid[i * RC : (i + 1) * RC, block(0, UNITS // 128 - 1)] = conv_part(UNITS // 128 - 1, i)

    def unit_share(t, rows):
        part = pl.ds(2 * t, 2)
        da = w[part, :, :, :, 0:DA].reshape(CH, DA)
        db = w[part, :, :, :, LA + UNITS : LW].reshape(CH, UNITS - DA)
        return dot_nt(hid[rows, 0:DA], da) + dot_nt(hid[rows, DA:UNITS], db)

    settle(sends[mark : mark + 6])
    early = len(sends)

    def settle_early():
        settle(d for d in sends[:mark] if d is not None)
        settle(sends[mark + 6 : early])
        copy_at(docs.at[0], docs.at[1], sib, "d1", S_ALT + 1).wait_send()
        copy_at(docs.at[0], docs.at[3], sib, "d3", S_ALT + 2).wait_send()
        copy_at(packs.at[2], packs.at[3], sib, "s3", S_ALT + 3).wait_send()

        @pl.when(c == 0)
        def _():
            copy_at(packs.at[0], packs.at[1], sib, "l1", S_ALT).wait_send()
            for i, at in enumerate(zero_only):
                part = quarter(3, 0, 0, QR if i < 2 else QR // 2)
                copy_at(part, part, yp, "l3", at).wait_send()

        @pl.when(c == 1)
        def _():
            copy_at(quarter(2, 0), quarter(3, 0), nexto, "l3", S_ALT).wait_send()

    far_all(unit_share, "u", ra2)
    near_all(unit_share, "u", rb2)
    own[...] = unit_share(y, pl.ds(0, ROWS))
    settle_early()
    forward("u", ra2, rb2)
    total_two = collected("u", rb2)
    mixed = (
        residual_scale * nf[LEAD : LEAD + ROWS, pl.ds(pl.multiple_of(y * CH, CH), CH)].astype(F32) + total_two
    )
    own[...] = mixed
    s = jnp.sum(mixed, axis=1, keepdims=True)
    q = jnp.sum(mixed * mixed, axis=1, keepdims=True)
    both = jnp.where(lane == 0, s, jnp.where(lane == 1, q, 0.0))
    stats[y] = both.T[0:8, :]
    same(stats.at[y], yp, "qm")
    same(stats.at[y], ym, "qp")
    same(stats.at[y], yy, "q2")
    settle(sends[early:])
    arrive(stats.at[wrap(y - 1, NY)], "qm")
    arrive(stats.at[wrap(y + 1, NY)], "qp")
    arrive(stats.at[wrap(y + 2, NY)], "q2")
    tot = (stats[0] + stats[1]) + (stats[2] + stats[3])
    back = jnp.concatenate([tot, jnp.zeros((120, ROWS), F32)], axis=0).T
    s = back[:, 0:1] / D
    q = back[:, 1:2] / D
    r = lax.rsqrt(q - s * s + norm_eps)
    out_ref[...] = ((own[...] - s) * r * gb_ref[2:3, :] + gb_ref[3:4, :]).astype(BF)


def local(
    residual, query_nope, query_rope, latent, rope_key, doc_ids, key_up, value_up, out_proj,
    norm1_gain, norm1_bias, ffn_gate, ffn_value, conv_gate, conv_value, ffn_down,
    norm2_gain, norm2_bias,
):
    rows = latent.shape[0]
    turn = rope_base_freq ** (-np.arange(0, ROPE, 2, dtype=np.float64) / ROPE)
    turn = jnp.asarray(np.tile(np.tile(turn, 4)[None], (8, 1)).astype(np.float32))

    anyspec = pl.BlockSpec(memory_space=pl.ANY)
    vspec = pl.BlockSpec(memory_space=pltpu.VMEM)
    V = pltpu.VMEM
    return pl.pallas_call(
        layer_kernel,
        out_shape=jax.ShapeDtypeStruct((rows, CH), BF),
        in_specs=[anyspec] * 19,
        out_specs=vspec,
        scratch_shapes=[
            V((ROPE, ROWS), BF),
            V((CH,), BF),
            V((CH,), BF),
            V((CH,), BF),
            V((CH,), BF),
            V((ROWS,), jnp.int32),
            V((CONV, UNITS), BF),
            V((CONV, UNITS), BF),
            V((8, 128), F32),
            V((8, CH), F32),
            V((ROWS, 128), F32),
            V((ROWS, 128), F32),
            V((4, ROWS, PACKW), BF),
            V((ROWS, 1024), BF),
            V((ROWS, CH), BF),
            V((ROWS, 1024), BF),
            V((512, 1024), BF),
            V((512, 1024), BF),
            V((1024, D), BF),
            V((ROWS, CH), BF),
            V((NZ, NX, 2, 32, LW), BF),
            V((NY, 8, CH), F32),
            V((ROWS, 1024), BF),
            V((8, ROWS, 128), F32),
            V((8, ROWS, 128), F32),
            V((8, ROWS, 128), F32),
            V((8 + ROWS, 128), F32),
            V((4, 8, ROWS), F32),
            V((ROWS, ROWS), F32),
            V((ROWS, CH), BF),
            V((ROWS, CH), BF),
            V((ROWS, CH), BF),
            V((HALF, CH), F32),
            V((HALF, CH), F32),
            V((ROWS, CH), F32),
            V((2, HALF, CH), BF),
            V((2, ROWS, CH), BF),
            V((2, HALF, CH), BF),
            V((2, ROWS, CH), BF),
            V((NY, ROWS, CH), BF),
            V((LEAD + ROWS, D), BF),
            V((LEAD + ROWS, 2 * UNITS), F32),
            V((ROWS, UNITS), BF),
            V((NY, LEAD, CH), BF),
            V((NY, 8, ROWS), F32),
            pltpu.SemaphoreType.DMA((24,)),
            pltpu.SemaphoreType.DMA((N_SEND,)),
            pltpu.SemaphoreType.DMA((N_RECV,)),
        ],
        compiler_params=pltpu.CompilerParams(
            collective_id=0, has_side_effects=True, vmem_limit_bytes=54 * 1024 * 1024
        ),
    )(
        latent, query_nope, query_rope, key_up, value_up, out_proj, residual,
        ffn_gate, ffn_value, ffn_down.T, rope_key.T, norm1_gain, norm1_bias, norm2_gain, norm2_bias,
        doc_ids, conv_gate, conv_value, turn,
    )


def solution(mesh):
    placed = (
        P("sp", "tp"),
        P("sp", "tp"),
        P("sp", "tp"),
        P("sp", None),
        P("sp", None),
        P("sp"),
        P(None, "tp"),
        P(None, "tp"),
        P("tp", None),
        P("tp"),
        P("tp"),
        P("sp", "tp"),
        P("sp", "tp"),
        P(None, "tp"),
        P(None, "tp"),
        P("tp", "sp"),
        P("tp"),
        P("tp"),
    )
    return jax.shard_map(
        local, mesh=mesh, in_specs=placed, out_specs=P("sp", "tp"), check_vma=False
    )
```
